256 devices in a mesh: sp: 64 (over z, y, core), tp: 4 (over x).
Axes of the slice: x: 4, y: 4, z: 8, core: 2. Of those that a mesh axis runs over, the one named last changes fastest.
Arguments:
- query_a: bfloat16 [8192, 1536], P('sp', 'tp'), may hold values from -400 to 400
- query_b: bfloat16 [8192, 2048], P('sp', 'tp'), may hold values from -400 to 400
- latent: bfloat16 [8192, 512], P(('sp', 'tp')), may hold values from -6 to 6
- rope_key: bfloat16 [8192, 64], P(('sp', 'tp')), may hold values from -6 to 6
- latent_gain: float32 [512], replicated, may hold values from 0.1 to 1.9
- key_a_weight: bfloat16 [512, 1024], P(None, 'tp'), may hold values from -0.25 to 0.25
- value_a_weight: bfloat16 [512, 1024], P(None, 'tp'), may hold values from -0.25 to 0.25
- key_b_weight: bfloat16 [512, 1024], P(None, 'tp'), may hold values from -0.25 to 0.25
- value_b_weight: bfloat16 [512, 1024], P(None, 'tp'), may hold values from -0.25 to 0.25
- out_a_weight: bfloat16 [1024, 2048], P('tp'), may hold values from -0.25 to 0.25
- out_b_weight: bfloat16 [1024, 2048], P('tp'), may hold values from -0.25 to 0.25
- residual: bfloat16 [8192, 2048], P(('sp', 'tp')), may hold values from -6 to 6
- ffn_gain: float32 [2048], replicated, may hold values from 0.1 to 1.9
- routes: int32 [8192, 2], P(('sp', 'tp')), may hold values from 0 to 63, all different within a row; in each aligned block of 32 rows (0 to 31, 32 to 63, ...) at most 2 rows name the same one
- route_weight: float32 [8192, 2], P(('sp', 'tp')), may hold values from 0.2 to 1
- expert_gate: bfloat16 [64, 2048, 3072], P('sp', None, 'tp'), may hold values from -0.125 to 0.125
- expert_up: bfloat16 [64, 2048, 3072], P('sp', None, 'tp'), may hold values from -0.125 to 0.125
- expert_down: bfloat16 [64, 3072, 2048], P('sp', 'tp'), may hold values from -0.109375 to 0.109375
Outputs:
- layer_out: bfloat16 [8192, 2048], P(('sp', 'tp'))
The draws below stay inside these ranges and needn't reach their ends.
Inputs may be any that keep to these rules, and one draw needn't show every extreme that they name: `routes`: the 2 experts of a row differ. Among the 32 rows of one device no expert is named more than 2 times, a bound that some block reaches in some devices' rows.
All inputs are finite; a program needn't handle non-finite values.
Results may differ from the reference program's by a relative error of at most 0.019.
The reference program's roundings to bfloat16 on the way count: a program that leaves them out, or rounds other values in their place, can miss the bound.
Values may be sent and summed in bfloat16 or wider, within the bound.
A program may use at most 128 MiB of HBM per device.

```python
import math
import jax
import jax.numpy as jnp
import numpy as np
from jax import lax

D = 2048
RANK = 512
ROPE = 64
HEADS_A = 8
NOPE_A = 128
VAL_A = 128
HEADS_B = 16
NOPE_B = 64
VAL_B = 64
FF = 3072
TOP = 2
TOKENS = 8192
ROWS = 32
EXPERTS = 64
CAP = 2
N_TP = 4


def query_table(key, columns):
    normal_part = jax.random.normal(jax.random.fold_in(key, 13), (TOKENS, columns), jnp.float32)
    return (3.0 * jnp.clip(normal_part, -4.0, 4.0)).astype(jnp.bfloat16)


def draw_query_a(key, part):
    return query_table(jax.random.fold_in(key, 1), HEADS_A * (NOPE_A + ROPE))


def draw_query_b(key, part):
    return query_table(jax.random.fold_in(key, 2), HEADS_B * (NOPE_B + ROPE))


def levels(stream_key, dims, pieces, low, high):
    gain, own = 1.0, jax.random.fold_in(stream_key, 6)
    for axis_at, parts in pieces:
        steps = jnp.exp(jax.random.uniform(jax.random.fold_in(own, axis_at), (parts,), jnp.float32, low / len(pieces), high / len(pieces)))
        gain = gain * jnp.repeat(steps, dims[axis_at] // parts).reshape([-1 if axis == axis_at else 1 for axis in range(len(dims))])
    return gain


def routed_block(key, own, number, rows, amount, top, reach, lean):
    order = jax.random.permutation(key, amount)
    packed, common = portions_of(amount, rows * top, reach, lean, True), portions_of(amount, rows * top, reach, lean, False)
    places = jnp.arange(amount)

    def named(sizes, offset_by):
        used = int((sizes > 0).sum())
        fixed = max(1, used // 4)
        passed = fixed + (places - fixed + offset_by * (used - fixed)) % max(1, amount - fixed)
        return jnp.zeros((amount,), jnp.int32).at[order[jnp.where(places < fixed, places, passed)]].set(jnp.asarray(sizes, jnp.int32))

    sizes = jnp.where(number % 4 == 0, named(packed, number // 4), named(common, number - number // 4 - 1))
    mixed = jax.random.permutation(jax.random.fold_in(own, 3), amount)
    source_of, taker = mixed[0:amount // 2 * 2:2], mixed[1:amount // 2 * 2:2]
    margin = jnp.minimum(sizes[source_of] - 1, reach - sizes[taker]) // 2
    margin = jnp.where((source_of == order[0]) | (taker == order[0]) | (sizes[taker] == 0), 0, jnp.maximum(margin, 0))
    passed = jax.random.randint(jax.random.fold_in(own, 4), (amount // 2,), 0, 1 << 20) % (margin + 1)
    sizes = sizes.at[source_of].add(-passed).at[taker].add(passed)
    items = jnp.searchsorted(jnp.cumsum(sizes), jnp.arange(rows * top), side="right").astype(jnp.int32)
    table = items.reshape(top, rows).T
    table = table[jax.random.permutation(jax.random.fold_in(own, 1), rows)]
    offset_by = jax.random.randint(jax.random.fold_in(own, 2), (rows, 1), 0, top)
    return jnp.take_along_axis(table, (jnp.arange(top)[None, :] + offset_by) % top, axis=1)


def portions_of(count, total, most, slope, full):
    portions = [(1 << 20) // math.isqrt(grade ** slope) + 1 for grade in range(1, count + 1)]
    largest = most if full else min(most, max(-(-total // count), total * portions[0] // sum(portions)))
    least = 1 if total - largest >= count - 1 else 0
    given, surplus = [largest] + [least] * (count - 1), total - largest - least * (count - 1)
    while surplus > 0:
        free = [i for i in range(1, count) if given[i] < largest] or [i for i in range(1, count) if given[i] < most]
        pool, left = sum([portions[i] for i in free]), surplus
        for i in free:
            extra = min(most - given[i], max(1, left * portions[i] // pool), surplus)
            given[i] = given[i] + extra
            surplus = surplus - extra
    return np.array(given)


def noise(own_key, dims, spread, limit, cuts=(), kind=jnp.bfloat16):
    factor_of = levels(own_key, dims, cuts, -0.22, 0.18) if cuts else 1.0
    values = jax.random.normal(own_key, dims, jnp.float32) * spread * factor_of
    return jnp.minimum(jnp.maximum(values, -limit), limit).astype(kind)


def setup_inputs(seed: int = 0) -> dict:
    key_list = jax.random.split(jax.random.key(seed), 19)
    query_a = draw_query_a(jax.random.fold_in(key_list[18], 71), 0)
    query_b = draw_query_b(jax.random.fold_in(key_list[18], 71), 0)
    latent = noise(key_list[2], (TOKENS, RANK), 1.0, 6.0, ((0, 256),))
    rope_key = noise(key_list[3], (TOKENS, ROPE), 1.0, 6.0, ((0, 256),))
    latent_gain = jnp.clip(1.0 + 0.18 * jax.random.normal(key_list[4], (RANK,), jnp.float32), 0.1, 1.9)
    key_a_weight = noise(key_list[5], (RANK, HEADS_A * NOPE_A), RANK ** -0.5, 0.25, ((1, 4),))
    value_a_weight = noise(key_list[6], (RANK, HEADS_A * VAL_A), RANK ** -0.5, 0.25, ((1, 4),))
    key_b_weight = noise(key_list[7], (RANK, HEADS_B * NOPE_B), RANK ** -0.5, 0.25, ((1, 4),))
    value_b_weight = noise(key_list[8], (RANK, HEADS_B * VAL_B), RANK ** -0.5, 0.25, ((1, 4),))
    out_a_weight = noise(key_list[9], (HEADS_A * VAL_A, D), (D // 4) ** -0.5, 0.25, ((0, 4),))
    out_b_weight = noise(key_list[10], (HEADS_B * VAL_B, D), (D // 4) ** -0.5, 0.25, ((0, 4),))
    residual = noise(key_list[11], (TOKENS, D), 1.0, 6.0, ((0, 256),))
    ffn_gain = jnp.clip(1.0 + 0.18 * jax.random.normal(key_list[12], (D,), jnp.float32), 0.1, 1.9)
    routes_keys = jax.random.split(jax.random.fold_in(key_list[13], 1), TOKENS // ROWS)
    routes_turns = jax.random.permutation(jax.random.fold_in(key_list[13], 3), TOKENS // ROWS)
    routes = jax.vmap(lambda own, number: routed_block(jax.random.fold_in(key_list[13], 2), own, number, ROWS, EXPERTS, TOP, CAP, 1))(routes_keys, routes_turns).reshape((TOKENS, TOP))
    route_weight = jnp.clip(jnp.exp(math.log(1.0) - 1.609438 * jax.random.uniform(key_list[14], (TOKENS, TOP), jnp.float32) ** levels(key_list[14], (TOKENS, TOP), ((0, 256),), -0.2, 0.2)), 0.2, 1.0)
    expert_gate = noise(key_list[15], (EXPERTS, D, FF), D ** -0.5, 0.125, ((0, 64), (2, 4)))
    expert_up = noise(key_list[16], (EXPERTS, D, FF), D ** -0.5, 0.125, ((0, 64), (2, 4)))
    expert_down = noise(key_list[17], (EXPERTS, FF, D), FF ** -0.5, 0.109375, ((0, 64), (1, 4)))
    return {"query_a": query_a, "query_b": query_b, "latent": latent, "rope_key": rope_key, "latent_gain": latent_gain, "key_a_weight": key_a_weight, "value_a_weight": value_a_weight, "key_b_weight": key_b_weight, "value_b_weight": value_b_weight, "out_a_weight": out_a_weight, "out_b_weight": out_b_weight, "residual": residual, "ffn_gain": ffn_gain, "routes": routes, "route_weight": route_weight, "expert_gate": expert_gate, "expert_up": expert_up, "expert_down": expert_down}


epsilon = 1e-06
base_theta = 500000.0

def rms_scale(values, scales):
    floats = values.astype(jnp.float32)
    scaled = floats * lax.rsqrt(lax.optimization_barrier(jnp.mean(floats * floats, axis=-1, keepdims=True)) + epsilon)
    return (scaled * scales).astype(jnp.bfloat16)

def angle_tables(positions, rotary_width):
    inverse = jnp.power(jnp.float32(base_theta), -jnp.arange(0, rotary_width, 2, dtype=jnp.float32) / rotary_width)
    angles = positions.astype(jnp.float32)[:, None] * inverse[None, :]
    return (jnp.cos(angles), jnp.sin(angles))

def rotate(values, cosine, sine_table):
    middle = cosine.shape[-1]
    first_half = values[..., :middle].astype(jnp.float32)
    second_half = values[..., middle:].astype(jnp.float32)
    turned = jnp.concatenate([first_half * cosine - second_half * sine_table, second_half * cosine + first_half * sine_table], axis=-1)
    return turned.astype(jnp.bfloat16)

def prepare_queries(queries, head_count, nope_width, cosine, sine_table):
    shaped = queries.reshape(queries.shape[0], head_count, queries.shape[1] // head_count)
    turned = rotate(shaped[:, :, nope_width:], cosine[:, None, :], sine_table[:, None, :])
    return jnp.concatenate([shaped[:, :, :nope_width], turned], axis=-1)

def attend(queries, keys, values):
    total_rows = queries.shape[0]
    block_rows = math.gcd(total_rows, 512)
    scale = queries.shape[-1] ** (-0.5)
    key_places = jnp.arange(total_rows, dtype=jnp.int32)
    keys_wide = keys.astype(jnp.float32)
    values_wide = values.astype(jnp.float32)

    def one_block(block_index):
        first_row = block_index * block_rows
        chosen_rows = lax.dynamic_slice_in_dim(queries, first_row, block_rows, 0).astype(jnp.float32)
        scores = jnp.einsum('thd,shd->hts', chosen_rows, keys_wide) * scale
        query_places = first_row + jnp.arange(block_rows, dtype=jnp.int32)
        allowed = (key_places[None, :] <= query_places[:, None])[None]
        scores = jnp.where(allowed, scores, -jnp.inf)
        highest = lax.optimization_barrier(jnp.max(scores, axis=-1, keepdims=True))
        weights = jnp.where(allowed, jnp.exp(scores - highest), 0.0)
        weight_total = lax.optimization_barrier(jnp.sum(weights, axis=-1))
        rounded = lax.optimization_barrier(weights.astype(jnp.bfloat16)).astype(jnp.float32)
        summed = jnp.einsum('hts,shd->thd', rounded, values_wide)
        return (summed / jnp.transpose(weight_total)[:, :, None]).astype(jnp.bfloat16)
    outputs = lax.map(one_block, jnp.arange(total_rows // block_rows))
    return outputs.reshape(total_rows, -1)

def experts_apply(normed, routes, expert_gate, expert_up, expert_down):
    total_rows = normed.shape[0]
    depth = total_rows // ROWS * CAP
    chosen = routes.reshape(-1).astype(jnp.int32)
    matches = (chosen[:, None] == jnp.arange(EXPERTS, dtype=jnp.int32)[None, :]).astype(jnp.int32)
    running = (jnp.cumsum(matches, axis=0).astype(jnp.int32) - 1) * matches
    order_rank = lax.optimization_barrier(jnp.sum(running, axis=1)).astype(jnp.int32)
    source_rows = jnp.repeat(jnp.arange(total_rows, dtype=jnp.int32), TOP)
    buffer = jnp.zeros((EXPERTS, depth, normed.shape[1]), jnp.bfloat16).at[chosen, order_rank].set(normed[source_rows])

    def one_expert(operands):
        arrived, gate_weight, up_weight, down_weight = operands
        gate_values = jnp.dot(arrived, gate_weight, preferred_element_type=jnp.float32)
        up_values = jnp.dot(arrived, up_weight, preferred_element_type=jnp.float32)
        hidden = (jax.nn.silu(gate_values) * up_values).astype(jnp.bfloat16)
        block_width = hidden.shape[1] // N_TP
        accumulated = jnp.zeros((arrived.shape[0], down_weight.shape[1]), jnp.float32)
        for block_index in range(N_TP):
            partial_value = jnp.dot(hidden[:, block_index * block_width:(block_index + 1) * block_width], down_weight[block_index * block_width:(block_index + 1) * block_width], preferred_element_type=jnp.float32).astype(jnp.bfloat16)
            accumulated = accumulated + lax.optimization_barrier(partial_value).astype(jnp.float32)
        return accumulated.astype(jnp.bfloat16)
    results = lax.map(one_expert, (buffer, expert_gate, expert_up, expert_down))
    return results[chosen, order_rank].reshape(total_rows, TOP, -1)

def reference(query_a, query_b, latent, rope_key, latent_gain, key_a_weight, value_a_weight, key_b_weight, value_b_weight, out_a_weight, out_b_weight, residual, ffn_gain, routes, route_weight, expert_gate, expert_up, expert_down):
    total_rows = residual.shape[0]
    positions = jnp.arange(total_rows, dtype=jnp.int32)
    cosine, sine_table = angle_tables(positions, ROPE)
    normed_latent = rms_scale(latent, latent_gain)
    turned_key = rotate(rope_key, cosine, sine_table)

    def expand(weight, head_count):
        product = jnp.dot(normed_latent, weight, preferred_element_type=jnp.float32).astype(jnp.bfloat16)
        return product.reshape(total_rows, head_count, weight.shape[1] // head_count)
    key_a = expand(key_a_weight, HEADS_A)
    value_a = expand(value_a_weight, HEADS_A)
    key_b = expand(key_b_weight, HEADS_B)
    value_b = expand(value_b_weight, HEADS_B)
    keys_a = jnp.concatenate([key_a, jnp.broadcast_to(turned_key[:, None, :], (total_rows, HEADS_A, ROPE))], axis=-1)
    keys_b = jnp.concatenate([key_b, jnp.broadcast_to(turned_key[:, None, :], (total_rows, HEADS_B, ROPE))], axis=-1)
    out_a = attend(prepare_queries(query_a, HEADS_A, NOPE_A, cosine, sine_table), keys_a, value_a)
    out_b = attend(prepare_queries(query_b, HEADS_B, NOPE_B, cosine, sine_table), keys_b, value_b)
    projected = jnp.dot(out_a, out_a_weight, preferred_element_type=jnp.float32) + jnp.dot(out_b, out_b_weight, preferred_element_type=jnp.float32)
    hidden_state = (residual.astype(jnp.float32) + projected).astype(jnp.bfloat16)
    normed = rms_scale(hidden_state, ffn_gain)
    picked = experts_apply(normed, routes, expert_gate, expert_up, expert_down).astype(jnp.float32)
    expert_mix = lax.optimization_barrier(jnp.sum(picked * route_weight[:, :, None], axis=1))
    return (hidden_state.astype(jnp.float32) + expert_mix).astype(jnp.bfloat16)
```

```python
import jax
import jax.numpy as jnp
from jax import lax
from jax.sharding import PartitionSpec as P

from jax.experimental import pallas as pl
from jax.experimental.pallas import tpu as pltpu


NOPE_A = 128
VAL_A = 128
NOPE_B = 64
VAL_B = 64
TOP = 2


epsilon = 1e-06
base_theta = 500000.0
masked_score = -1e30


def rms_scale(values, scales):
    floats = values.astype(jnp.float32)
    scaled = floats * lax.rsqrt(jnp.mean(floats * floats, axis=-1, keepdims=True) + epsilon)
    return (scaled * scales).astype(jnp.bfloat16)


def angle_tables(positions, rotary_width):
    inverse = jnp.power(
        jnp.float32(base_theta), -jnp.arange(0, rotary_width, 2, dtype=jnp.float32) / rotary_width
    )
    angles = positions.astype(jnp.float32)[:, None] * inverse[None, :]
    return (jnp.cos(angles), jnp.sin(angles))


def rotate(values, cosine, sine_table):
    middle = cosine.shape[-1]
    first_half = values[..., :middle].astype(jnp.float32)
    second_half = values[..., middle:].astype(jnp.float32)
    turned = jnp.concatenate(
        [
            first_half * cosine - second_half * sine_table,
            second_half * cosine + first_half * sine_table,
        ],
        axis=-1,
    )
    return turned.astype(jnp.bfloat16)


LOG2E = 1.4426950408889634
MESH_ID = pl.DeviceIdType.MESH
NZ, NY, NX = 8, 4, 4


def place():
    sp = lax.axis_index("sp")
    return sp // 8, (sp // 2) % 4, sp % 2, lax.axis_index("tp")


def send(src, dst, send_sem, recv_sem, z, y, c, x):
    return pltpu.make_async_remote_copy(
        src_ref=src,
        dst_ref=dst,
        send_sem=send_sem,
        recv_sem=recv_sem,
        device_id=(z * 8 + y * 2 + c, x),
        device_id_type=MESH_ID,
    )


def nt_dot(a, b):
    return lax.dot_general(a, b, (((1,), (1,)), ((), ())), preferred_element_type=jnp.float32)


def attention_kernel(
    lat_ref, q_ref, ka_ref, kb_ref, va_ref, vb_ref, oa_ref, ob_ref, res_ref, hid_ref,
    latg, qg, w, wo, k_a, k_b0, k_b1, val, scores, o_out, o_in, st_out, st_in, mg, mg_in, pj, pj_in,
    w_sem, zs, zr, xs, xr, ms, mr, qs, qr, os_, or_, ss, sr, gs, gr, ps, pr,
):
    z, y, c, x = place()
    mate = 1 - c
    low = pl.multiple_of(c * 128, 128)
    high = pl.multiple_of(mate * 128, 128)

    loads = [
        pltpu.make_async_copy(r.at[:, pl.ds(low, 128)], w.at[:, pl.ds(i * 128, 128)], w_sem.at[i])
        for i, r in enumerate((ka_ref, kb_ref, va_ref, vb_ref))
    ]
    for i, at in enumerate((low, high)):
        for j, r in enumerate((oa_ref, ob_ref)):
            loads.append(
                pltpu.make_async_copy(
                    r.at[pl.ds(at, 128), :], wo.at[i, pl.ds(j * 128, 128)], w_sem.at[4 + 2 * i + j]
                )
            )
    for load in loads:
        load.start()

    barrier = pltpu.get_barrier_semaphore()

    def greet(pz, py, pc, px):
        pl.semaphore_signal(
            barrier, inc=1, device_id=(pz * 8 + py * 2 + pc, px), device_id_type=MESH_ID
        )

    for d in range(1, NZ):
        greet((z + d) % NZ, y, c, x)
    for d in range(1, NX):
        greet(z, y, c, (x + d) % NX)
    for dy in range(NY):
        for dc in range(2):
            if dy or dc:
                greet(z, (y + dy) % NY, (c + dc) % 2, x)
    pl.semaphore_wait(barrier, NZ - 1 + NX - 1 + 2 * NY - 1)

    own_rows = pl.ds(pl.multiple_of(c * 128 + x * 32, 32), 32)
    core_rows = pl.ds(low, 128)
    sends = []

    z_sends = [None]
    for d in range(1, NZ):
        z_sends.append(
            send(lat_ref, latg.at[d, own_rows], zs.at[d], zr.at[d], (z + d) % NZ, y, c, x)
        )
    for d in (4, 3, 5, 2, 6, 1, 7):
        z_sends[d].start()
    latg[0, own_rows] = lat_ref[...]

    def x_send(d, dx):
        src = lat_ref if d == 0 else latg.at[d, own_rows]
        return send(src, latg.at[d, own_rows], xs.at[d, dx], xr.at[d, dx], z, y, c, (x + dx) % NX)

    x_sends = [[x_send(d, dx) for dx in range(1, NX)] for d in range(NZ)]
    for dx in range(3):
        x_sends[0][dx].start()

    q_sends = []
    for dy in (2, 1, 3, 0):
        for dc in range(2):
            if dy == 0 and dc == 0:
                continue
            pc = (c + dc) % 2
            q_sends.append(
                send(
                    q_ref.at[pc], qg.at[dy, core_rows], qs.at[dy, dc], qr.at[dy, dc],
                    z, (y + dy) % NY, pc, x,
                )
            )
            q_sends[-1].start()
    qg[0, core_rows] = q_ref[c]

    order = (1, 7, 2, 6, 3, 5, 4)
    for d in order:
        z_sends[d].wait_recv()
        for dx in range(3):
            x_sends[d][dx].start()
    m_sends = [
        send(latg.at[d, core_rows], latg.at[d, core_rows], ms.at[d], mr.at[d], z, y, mate, x)
        for d in range(NZ)
    ]
    for d in (0,) + order:
        for dx in range(3):
            x_sends[d][dx].wait_recv()
        m_sends[d].start()

    for load in loads[:4]:
        load.wait()
    lane = lax.broadcasted_iota(jnp.int32, (256, 128), 1)
    for d in (0,) + order:
        m_sends[d].wait_recv()
        block = latg[d]
        made = jnp.dot(block[:, :512], w[...], preferred_element_type=jnp.float32)
        made = made.astype(jnp.bfloat16)
        turned = block[:, 512:]
        b = made[:, 128:256]
        k_a[d, :, :128] = made[:, :128]
        k_a[d, :, 128:] = turned
        k_b0[d] = jnp.where(lane < 64, b, turned)
        k_b1[d] = jnp.where(lane < 64, turned, b)
        val[d] = made[:, 256:]
    for s in q_sends:
        s.wait_recv()

    factors = (LOG2E * 192**-0.5, LOG2E * 128**-0.5, LOG2E * 128**-0.5)
    row = lax.broadcasted_iota(jnp.int32, (256, 256), 0)
    col = lax.broadcasted_iota(jnp.int32, (256, 256), 1)

    def raw_scores(dy, d):
        q = qg[dy]
        return (
            nt_dot(q[:, :256], k_a[d]),
            nt_dot(q[:, 256:384], k_b0[d]),
            nt_dot(q[:, 384:], k_b1[d]),
        )

    def attend(dy, _):
        chip = (y - dy + NY) % NY
        allowed = row + (chip - y) * 256 >= col
        tops = []
        for h, s in enumerate(raw_scores(dy, 0)):
            s = jnp.where(allowed, s, -1e30)
            scores[h, 0] = s
            tops.append(jnp.maximum(s[:, :128], s[:, 128:]))

        def first(d, tops):
            new = []
            for h, s in enumerate(raw_scores(dy, d)):
                scores[h, d] = s
                new.append(jnp.maximum(tops[h], jnp.maximum(s[:, :128], s[:, 128:])))
            return tuple(new)

        tops = lax.fori_loop(1, z + 1, first, tuple(tops))
        tops = [jnp.max(t, axis=1, keepdims=True) for t in tops]

        def second(d, carried):
            new = []
            v = val[d]
            for h in range(3):
                total, acc = carried[h]
                p = jnp.exp2((scores[h, d] - tops[h]) * factors[h])
                total = total + (p[:, :128] + p[:, 128:])
                vh = v[:, :128] if h == 0 else v[:, 128:]
                acc = acc + jnp.dot(
                    p.astype(jnp.bfloat16), vh, preferred_element_type=jnp.float32
                )
                new.append((total, acc))
            return tuple(new)

        zero = jnp.zeros((256, 128), jnp.float32)
        done = lax.fori_loop(0, z + 1, second, ((zero, zero),) * 3)
        outs, lses = [], []
        for h in range(3):
            total = jnp.sum(done[h][0], axis=1, keepdims=True)
            outs.append(done[h][1] / total)
            lses.append(tops[h] * factors[h] + jnp.log2(total))
        o_out[dy, :, :128] = outs[0].astype(jnp.bfloat16)
        o_out[dy, :, 128:] = jnp.where(lane < 64, outs[1], outs[2]).astype(jnp.bfloat16)
        stats = jnp.where(lane == 0, lses[0], jnp.where(lane == 1, lses[1], lses[2]))
        st_out[dy] = jnp.transpose(stats)[:8]
        return 0

    def o_send(dy):
        return send(
            o_out.at[dy], o_in.at[dy], os_.at[dy], or_.at[dy], z, (y - dy + NY) % NY, c, x
        ), send(st_out.at[dy], st_in.at[dy], ss.at[dy], sr.at[dy], z, (y - dy + NY) % NY, c, x)

    o_sends = []
    for dy in (2, 1, 3, 0):
        attend(dy, 0)
        if dy:
            o_sends.extend(o_send(dy))
            for s in o_sends[-2:]:
                s.start()
    for s in o_sends:
        s.wait_recv()

    lse = [jnp.transpose(st_out[0])] + [jnp.transpose(st_in[dy]) for dy in range(1, NY)]
    top = jnp.maximum(jnp.maximum(lse[0], lse[1]), jnp.maximum(lse[2], lse[3]))
    weights = [jnp.exp2(v - top) for v in lse]
    inv = 1.0 / (weights[0] + weights[1] + weights[2] + weights[3])
    sum_a = jnp.zeros((256, 128), jnp.float32)
    sum_b = jnp.zeros((256, 128), jnp.float32)
    for dy in range(NY):
        part = (o_out[0] if dy == 0 else o_in[dy]).astype(jnp.float32)
        wt = weights[dy] * inv
        sum_a = sum_a + part[:, :128] * wt[:, 0:1]
        sum_b = sum_b + part[:, 128:] * jnp.where(lane < 64, wt[:, 1:2], wt[:, 2:3])
    mg[:, :128] = sum_a.astype(jnp.bfloat16)
    mg[:, 128:] = sum_b.astype(jnp.bfloat16)
    swap = send(mg.at[pl.ds(high, 128)], mg_in, gs, gr, z, y, mate, x)
    swap.start()
    for load in loads[4:]:
        load.wait()
    swap.wait_recv()
    made = jnp.dot(mg[core_rows], wo[0], preferred_element_type=jnp.float32)
    made = made + jnp.dot(mg_in[...], wo[1], preferred_element_type=jnp.float32)
    pj[...] = made.astype(jnp.bfloat16)
    p_sends = []
    for dx in (2, 1, 3):
        to = (x + dx) % NX
        p_sends.append(
            send(
                pj.at[pl.ds(pl.multiple_of(to * 32, 32), 32)], pj_in.at[dx], ps.at[dx], pr.at[dx],
                z, y, c, to,
            )
        )
        p_sends[-1].start()
    total = pj[pl.ds(pl.multiple_of(x * 32, 32), 32)].astype(jnp.float32)
    for s in p_sends:
        s.wait_recv()
    for dx in range(1, NX):
        total = total + pj_in[dx].astype(jnp.float32)
    hid_ref[...] = (res_ref[...].astype(jnp.float32) + total).astype(jnp.bfloat16)

    for s in z_sends[1:] + [s for part in x_sends for s in part] + m_sends + q_sends:
        s.wait_send()
    for s in o_sends + [swap] + p_sends:
        s.wait_send()


def attention(latent_rows, queries, weights, residual):
    vm = pl.BlockSpec(memory_space=pltpu.VMEM)
    hbm = pl.BlockSpec(memory_space=pl.ANY)
    bf, f32 = jnp.bfloat16, jnp.float32
    dma = pltpu.SemaphoreType.DMA
    return pl.pallas_call(
        attention_kernel,
        out_shape=jax.ShapeDtypeStruct(residual.shape, bf),
        in_specs=[vm, vm] + [hbm] * 6 + [vm],
        out_specs=vm,
        scratch_shapes=[
            pltpu.VMEM((8, 256, 640), bf),
            pltpu.VMEM((4, 256, 512), bf),
            pltpu.VMEM((512, 512), bf),
            pltpu.VMEM((2, 256, 2048), bf),
            pltpu.VMEM((8, 256, 256), bf),
            pltpu.VMEM((8, 256, 128), bf),
            pltpu.VMEM((8, 256, 128), bf),
            pltpu.VMEM((8, 256, 256), bf),
            pltpu.VMEM((3, 8, 256, 256), f32),
            pltpu.VMEM((4, 256, 256), bf),
            pltpu.VMEM((4, 256, 256), bf),
            pltpu.VMEM((4, 8, 256), f32),
            pltpu.VMEM((4, 8, 256), f32),
            pltpu.VMEM((256, 256), bf),
            pltpu.VMEM((128, 256), bf),
            pltpu.VMEM((128, 2048), bf),
            pltpu.VMEM((4, 32, 2048), bf),
            dma((8,)),
            dma((8,)), dma((8,)),
            dma((8, 4)), dma((8, 4)),
            dma((8,)), dma((8,)),
            dma((4, 2)), dma((4, 2)),
            dma((4,)), dma((4,)),
            dma((4,)), dma((4,)),
            dma, dma,
            dma((4,)), dma((4,)),
        ],
        compiler_params=pltpu.CompilerParams(
            collective_id=0, has_side_effects=True, vmem_limit_bytes=48 * 1024 * 1024
        ),
        cost_estimate=pl.CostEstimate(flops=8 * 10**9, bytes_accessed=8 * 10**6, transcendentals=0),
    )(latent_rows, queries, *weights, residual)


def core_queries(query_a, query_b, cosine, sine_table):
    rows = query_a.shape[0]
    a = query_a.reshape(rows, 2, 192)
    b = query_b.reshape(rows, 4, 128)
    turned_a = rotate(a[:, :, NOPE_A:], cosine[:, None, :], sine_table[:, None, :])
    turned_b = rotate(b[:, :, NOPE_B:], cosine[:, None, :], sine_table[:, None, :])
    empty = jnp.zeros((rows, 64), jnp.bfloat16)
    halves = []
    for c in range(2):
        halves.append(
            jnp.concatenate(
                [
                    a[:, c, :NOPE_A], turned_a[:, c], empty,
                    b[:, 2 * c, :NOPE_B], turned_b[:, 2 * c],
                    turned_b[:, 2 * c + 1], b[:, 2 * c + 1, :NOPE_B],
                ],
                axis=-1,
            )
        )
    return jnp.stack(halves)


def body(
    query_a,
    query_b,
    latent,
    rope_key,
    latent_gain,
    key_a_weight,
    value_a_weight,
    key_b_weight,
    value_b_weight,
    out_a_weight,
    out_b_weight,
    residual,
    ffn_gain,
    routes,
    route_weight,
    expert_gate,
    expert_up,
    expert_down,
):
    column_count = lax.axis_size("tp")
    row_count = latent.shape[0]
    span_size = query_a.shape[0]
    rotary_width = rope_key.shape[1]
    own_first = (lax.axis_index("sp") * column_count + lax.axis_index("tp")) * row_count
    query_first = lax.axis_index("sp") * span_size
    last_query = query_first + span_size - 1
    own_cosine, own_sine = angle_tables(
        own_first + jnp.arange(row_count, dtype=jnp.int32), rotary_width
    )
    normed_latent = rms_scale(latent, latent_gain)
    turned_key = rotate(rope_key, own_cosine, own_sine)
    query_cosine, query_sine = angle_tables(
        query_first + jnp.arange(span_size, dtype=jnp.int32), rotary_width
    )
    queries = core_queries(query_a, query_b, query_cosine, query_sine)
    latent_rows = jnp.concatenate([normed_latent, turned_key, turned_key], axis=-1)
    hidden_state = attention(
        latent_rows,
        queries,
        (key_a_weight, key_b_weight, value_a_weight, value_b_weight, out_a_weight, out_b_weight),
        residual,
    )
    normed = rms_scale(hidden_state, ffn_gain)
    model_width = normed.shape[1]
    experts = lax.axis_size("sp")
    capacity = max(2, 2 * TOP * row_count // experts)
    chosen = routes.reshape(-1)
    expert_ids = jnp.arange(experts, dtype=jnp.int32)
    matches = (chosen[:, None] == expert_ids[None, :]).astype(jnp.int32)
    order_rank = jnp.sum((jnp.cumsum(matches, axis=0) - 1) * matches, axis=1)
    slot_index = (chosen * capacity + order_rank).reshape(row_count, TOP)
    slot_ids = jnp.arange(experts * capacity, dtype=jnp.int32)
    selection = jnp.sum(
        (slot_ids[:, None, None] == slot_index[None, :, :]).astype(jnp.bfloat16), axis=2
    )
    outgoing = jnp.dot(selection, normed, preferred_element_type=jnp.float32).astype(jnp.bfloat16)
    outgoing = outgoing.reshape(experts, capacity, model_width)
    portion = lax.all_gather(
        lax.all_to_all(outgoing, "sp", split_axis=0, concat_axis=0, tiled=True),
        "tp",
        axis=1,
        tiled=True,
    )
    portion_shape = portion.shape
    flat_rows = portion.reshape(portion_shape[0] * portion_shape[1], portion_shape[2])
    gate_values = jnp.dot(flat_rows, expert_gate[0], preferred_element_type=jnp.float32)
    up_values = jnp.dot(flat_rows, expert_up[0], preferred_element_type=jnp.float32)
    hidden = (jax.nn.silu(gate_values) * up_values).astype(jnp.bfloat16)
    partial_value = jnp.dot(hidden, expert_down[0], preferred_element_type=jnp.float32).astype(
        jnp.bfloat16
    )
    partials = lax.optimization_barrier(partial_value).astype(jnp.float32).reshape(portion_shape)
    summed = lax.psum_scatter(partials.astype(jnp.bfloat16), "tp", scatter_dimension=1, tiled=True)
    returned = lax.all_to_all(summed, "sp", split_axis=0, concat_axis=0, tiled=True)
    flat_returned = returned.reshape(experts * capacity, model_width)
    expert_mix = jnp.zeros((row_count, model_width), jnp.float32)
    for route_index in range(TOP):
        selector = (slot_index[:, route_index][:, None] == slot_ids[None, :]).astype(jnp.bfloat16)
        picked = jnp.dot(selector, flat_returned, preferred_element_type=jnp.float32)
        expert_mix = expert_mix + route_weight[:, route_index][:, None] * picked
    return (hidden_state.astype(jnp.float32) + expert_mix).astype(jnp.bfloat16)


def solution(mesh):
    placed = (
        P("sp", "tp"),
        P("sp", "tp"),
        P(("sp", "tp"), None),
        P(("sp", "tp"), None),
        P(),
        P(None, "tp"),
        P(None, "tp"),
        P(None, "tp"),
        P(None, "tp"),
        P("tp", None),
        P("tp", None),
        P(("sp", "tp"), None),
        P(),
        P(("sp", "tp"), None),
        P(("sp", "tp"), None),
        P("sp", None, "tp"),
        P("sp", None, "tp"),
        P("sp", "tp", None),
    )
    return jax.shard_map(
        body, mesh=mesh, in_specs=placed, out_specs=P(("sp", "tp"), None), check_vma=False
    )
```

```python
import jax
import jax.numpy as jnp
import numpy as np
from jax import lax
from jax.experimental import pallas as pl
from jax.experimental.pallas import tpu as pltpu
from jax.sharding import PartitionSpec as P

NZ, NY, NX = 8, 4, 4
TOKENS_PER_SP = 128
ROWS = 32
CHUNKS = 4
WIDE = 512
LOG2E = 1.4426950408889634
EPSILON = 1e-06
BASE_THETA = 500000.0
MASKED = -1e30
MESH_ID = pl.DeviceIdType.MESH
BF, F32 = jnp.bfloat16, jnp.float32


def angle_tables():
    inverse = BASE_THETA ** (-np.arange(0, 64, 2, dtype=np.float64) / 64)
    lanes = np.tile(inverse, 4)[None, :]

    def table(positions):
        angles = positions[:, None] * lanes
        return np.concatenate([np.cos(angles), np.sin(angles)], axis=1).astype(np.float32)

    return table(np.arange(64) * 128.0), table(np.arange(128) * 1.0)


def send(src, dst, send_sem, recv_sem, z, y, c, x):
    return pltpu.make_async_remote_copy(
        src_ref=src,
        dst_ref=dst,
        send_sem=send_sem,
        recv_sem=recv_sem,
        device_id=(z * 8 + y * 2 + c, x),
        device_id_type=MESH_ID,
    )


def dot(a, b):
    return jnp.dot(a, b, preferred_element_type=F32)


def nt_dot(a, b):
    return lax.dot_general(a, b, (((1,), (1,)), ((), ())), preferred_element_type=F32)


def iota(shape, dim):
    return lax.broadcasted_iota(jnp.int32, shape, dim)


def layer_kernel(
    qa_ref, qb_ref, lat_ref, rope_ref, gain_ref, ka_ref, va_ref, kb_ref, vb_ref, oa_ref, ob_ref,
    res_ref, fg_ref, rt_ref, wt_ref, eg_ref, eu_ref, ed_ref, ta_ref, tb_ref,
    out_ref,
    qa, qb, lat, rope, gain, res, fg, rt, wt, ta, tb,
    lat_own, q_own, latg, qg, w, wo, k_a, k_b0, k_b1, val, scores, o_out, o_in, st_out, st_in,
    mg, mg_in, pj, pj_half, pj_in,
    wg, wu, wd, disp, z_in, y_out, x_in, acc_g, acc_u, act, p_out, p_half, p_in, r_sum, ry_in,
    rz_out, rz_in,
    in_sem, w_sem, zs, zr, xs, xr, ms, mr, qs, qr, os_, or_, ss, sr, gs, gr, ps, pr,
    dzs, dzr, dys, dyr, dxs, dxr, rxs, rxr, rys, ryr, rzs, rzr,
):
    sp = lax.axis_index("sp")
    x = lax.axis_index("tp")
    z, y, c = sp // 8, (sp // 2) % 4, sp % 2
    mate = 1 - c
    low = pl.multiple_of(c * 128, 128)
    high = pl.multiple_of(mate * 128, 128)
    up = (x + 1) % NX
    down = (x + NX - 1) % NX

    def zp(d):
        return (z + d + NZ) % NZ

    def yp(d):
        return (y + d + NY) % NY

    def xp(d):
        return (x + d + NX) % NX

    small = [
        pltpu.make_async_copy(src, dst, in_sem.at[i])
        for i, (src, dst) in enumerate(
            (
                (lat_ref, lat), (rope_ref, rope), (gain_ref, gain), (ta_ref, ta), (tb_ref, tb),
                (qa_ref, qa), (qb_ref, qb), (res_ref, res), (fg_ref, fg), (rt_ref, rt), (wt_ref, wt),
            )
        )
    ]
    for load in small:
        load.start()
    loads = [
        pltpu.make_async_copy(r.at[:, pl.ds(low, 128)], w.at[:, pl.ds(i * 128, 128)], w_sem.at[i])
        for i, r in enumerate((ka_ref, kb_ref, va_ref, vb_ref))
    ]
    for i, at in enumerate((low, high)):
        for j, r in enumerate((oa_ref, ob_ref)):
            loads.append(
                pltpu.make_async_copy(
                    r.at[pl.ds(at, 128), :], wo.at[i, pl.ds(j * 128, 128)], w_sem.at[4 + 2 * i + j]
                )
            )
    for i, (src, dst) in enumerate(((eg_ref, wg), (eu_ref, wu), (ed_ref, wd))):
        loads.append(pltpu.make_async_copy(src.at[0], dst, w_sem.at[8 + i]))
    for load in loads:
        load.start()

    barrier = pltpu.get_barrier_semaphore()

    def greet(pz, py, pc, px):
        pl.semaphore_signal(
            barrier, inc=1, device_id=(pz * 8 + py * 2 + pc, px), device_id_type=MESH_ID
        )

    for d in range(1, NZ):
        greet(zp(d), y, c, x)
    for d in range(1, NX):
        greet(z, y, c, xp(d))
    for dy in range(NY):
        for dc in range(2):
            if dy or dc:
                greet(z, yp(dy), (c + dc) % 2, x)

    for load in small[:5]:
        load.wait()
    v = lat[...].astype(F32)
    v = v * lax.rsqrt(jnp.mean(v * v, axis=1, keepdims=True) + EPSILON)
    lat_own[:, :512] = (v * gain[...]).astype(BF)
    base = jnp.sum(jnp.where(iota((64, 256), 0) == sp, ta[...], 0.0), axis=0, keepdims=True)
    cos_a, sin_a = base[:, :128], base[:, 128:]

    def turning(cos_b, sin_b):
        lane = iota(cos_b.shape, 1)
        sine = sin_a * cos_b + cos_a * sin_b
        return cos_a * cos_b - sin_a * sin_b, jnp.where(lane % 64 < 32, -sine, sine)

    def rotated(tile, cosine, sine):
        lane = iota(tile.shape, 1)
        other = jnp.where(
            lane % 64 < 32, pltpu.roll(tile, 96, axis=1), pltpu.roll(tile, 32, axis=1)
        )
        return tile * cosine + other * sine

    own_32 = pl.ds(pl.multiple_of(x * ROWS, ROWS), ROWS)
    cosine, sine = turning(tb[own_32, :128], tb[own_32, 128:])
    twice = (iota((64, 128), 1) % 64 == iota((64, 128), 0)).astype(BF)
    lat_own[:, 512:] = rotated(dot(rope[...], twice), cosine, sine).astype(BF)

    pl.semaphore_wait(barrier, NZ - 1 + NX - 1 + 2 * NY - 1)

    def rows_of(px, at, count):
        return pl.ds(pl.multiple_of(c * 128 + px * ROWS + at, 16), count)

    core_rows = pl.ds(low, 128)
    all_sends = []

    z_sends = [None] + [
        send(lat_own, latg.at[d, rows_of(x, 0, 32)], zs.at[d], zr.at[d], zp(d), y, c, x)
        for d in range(1, NZ)
    ]
    all_sends += z_sends[1:]

    def ring(d):
        own = lat_own if d == 0 else latg.at[d, rows_of(x, 0, 32)]
        to = latg.at[d, rows_of(x, 0, 32)]
        one = latg.at[d, rows_of(down, 0, 16)]
        two = latg.at[d, rows_of(up, 16, 16)]
        return (
            send(own, to, xs.at[d, 0], xr.at[d, 0], z, y, c, up),
            send(own, to, xs.at[d, 1], xr.at[d, 1], z, y, c, down),
            send(one, one, xs.at[d, 2], xr.at[d, 2], z, y, c, up),
            send(two, two, xs.at[d, 3], xr.at[d, 3], z, y, c, down),
        )

    x_sends = [ring(d) for d in range(NZ)]
    for d in range(NZ):
        all_sends += x_sends[d]
    x_sends[0][0].start()
    x_sends[0][1].start()
    for d in (1, 7, 2, 6, 3, 5, 4):
        z_sends[d].start()
    latg[0, rows_of(x, 0, 32)] = lat_own[...]

    small[5].wait()
    small[6].wait()
    cosine, sine = turning(tb[:, :128], tb[:, 128:])
    lane = iota((128, 128), 1)
    t1 = qa[:, 128:256]
    t2 = qa[:, 256:384]
    r1 = rotated(t1.astype(F32), cosine, sine)
    r2 = rotated(t2.astype(F32), cosine, sine)
    mixed = jnp.where(lane < 64, t2.astype(F32), t1.astype(F32))
    q_own[0, :, :128] = qa[:, :128]
    q_own[0, :, 128:256] = jnp.where(lane < 64, r1, 0.0).astype(BF)
    q_own[1, :, :128] = pltpu.roll(mixed, 64, axis=1).astype(BF)
    q_own[1, :, 128:256] = jnp.where(lane < 64, 0.0, r2).astype(BF)
    for h in range(4):
        t = qb[:, h * 128 : h * 128 + 128].astype(F32)
        t = jnp.where(lane < 64, t, rotated(t, cosine, sine))
        if h % 2:
            t = pltpu.roll(t, 64, axis=1)
        q_own[h // 2, :, 256 + (h % 2) * 128 : 384 + (h % 2) * 128] = t.astype(BF)

    q_sends = []
    for dc in range(2):
        pc = (c + dc) % 2
        there = pl.ds(pl.multiple_of(pc * 128, 128), 128)
        one = qg.at[1, pl.ds(pl.multiple_of(pc * 128, 64), 64)]
        one_to = qg.at[2, pl.ds(pl.multiple_of(pc * 128, 64), 64)]
        two = qg.at[3, pl.ds(pl.multiple_of(pc * 128 + 64, 64), 64)]
        two_to = qg.at[2, pl.ds(pl.multiple_of(pc * 128 + 64, 64), 64)]
        q_sends.append(
            (
                send(q_own.at[pc], qg.at[1, core_rows], qs.at[dc, 0], qr.at[dc, 0], z, yp(1), pc, x),
                send(q_own.at[pc], qg.at[3, core_rows], qs.at[dc, 1], qr.at[dc, 1], z, yp(-1), pc, x),
                send(one, one_to, qs.at[dc, 2], qr.at[dc, 2], z, yp(1), c, x),
                send(two, two_to, qs.at[dc, 3], qr.at[dc, 3], z, yp(-1), c, x),
            )
        )
    q_mate = send(q_own.at[mate], qg.at[0, core_rows], qs.at[0, 4], qr.at[0, 4], z, y, mate, x)
    all_sends += q_sends[0] + q_sends[1] + (q_mate,)
    for dc in range(2):
        q_sends[dc][0].start()
        q_sends[dc][1].start()
    q_mate.start()
    qg[0, core_rows] = q_own[c]

    m_sends = [
        send(latg.at[d, core_rows], latg.at[d, core_rows], ms.at[d], mr.at[d], z, y, mate, x)
        for d in range(NZ)
    ]
    all_sends += m_sends

    def forward(d):
        x_sends[d][0].wait_recv()
        x_sends[d][2].start()
        x_sends[d][1].wait_recv()
        x_sends[d][3].start()

    def to_mate(d):
        x_sends[d][2].wait_recv()
        x_sends[d][3].wait_recv()
        m_sends[d].start()

    order = (1, 7, 2, 6, 3, 5, 4)
    steps = (0,) + order
    for i in range(len(steps) + 2):
        if i + 1 < len(steps):
            d = steps[i + 1]
            z_sends[d].wait_recv()
            x_sends[d][0].start()
            x_sends[d][1].start()
        if i < len(steps):
            forward(steps[i])
        if 1 <= i <= len(steps):
            to_mate(steps[i - 1])
        if i in (1, 2):
            dc = i - 1
            q_sends[dc][0].wait_recv()
            q_sends[dc][2].start()
            q_sends[dc][1].wait_recv()
            q_sends[dc][3].start()

    for load in loads[:4]:
        load.wait()
    lane = iota((256, 128), 1)
    for d in steps:
        m_sends[d].wait_recv()
        block = latg[d]
        made = dot(block[:, :512], w[...]).astype(BF)
        turned = block[:, 512:]
        b = made[:, 128:256]
        k_a[d, :, :128] = made[:, :128]
        k_a[d, :, 128:] = turned
        k_b0[d] = jnp.where(lane < 64, b, turned)
        k_b1[d] = jnp.where(lane < 64, turned, b)
        val[d] = made[:, 256:]
    q_mate.wait_recv()
    for dc in range(2):
        q_sends[dc][2].wait_recv()
        q_sends[dc][3].wait_recv()

    factors = (LOG2E * 192**-0.5, LOG2E * 128**-0.5, LOG2E * 128**-0.5)
    row = iota((256, 256), 0)
    col = iota((256, 256), 1)

    def raw_scores(dy, d):
        q = qg[dy]
        return (
            nt_dot(q[:, :256], k_a[d]),
            nt_dot(q[:, 256:384], k_b0[d]),
            nt_dot(q[:, 384:], k_b1[d]),
        )

    def attend(dy):
        allowed = row + (yp(-dy) - y) * 256 >= col
        tops = []
        for h, s in enumerate(raw_scores(dy, 0)):
            s = jnp.where(allowed, s, MASKED)
            scores[h, 0] = s
            tops.append(jnp.maximum(s[:, :128], s[:, 128:]))

        def first(d, tops):
            new = []
            for h, s in enumerate(raw_scores(dy, d)):
                scores[h, d] = s
                new.append(jnp.maximum(tops[h], jnp.maximum(s[:, :128], s[:, 128:])))
            return tuple(new)

        tops = lax.fori_loop(1, z + 1, first, tuple(tops))
        tops = [jnp.max(t, axis=1, keepdims=True) for t in tops]

        def second(d, carried):
            new = []
            values = val[d]
            for h in range(3):
                total, acc = carried[h]
                p = jnp.exp2((scores[h, d] - tops[h]) * factors[h])
                total = total + (p[:, :128] + p[:, 128:])
                acc = acc + dot(p.astype(BF), values[:, :128] if h == 0 else values[:, 128:])
                new.append((total, acc))
            return tuple(new)

        zero = jnp.zeros((256, 128), F32)
        done = lax.fori_loop(0, z + 1, second, ((zero, zero),) * 3)
        outs, lses = [], []
        for h in range(3):
            total = jnp.sum(done[h][0], axis=1, keepdims=True)
            outs.append(done[h][1] / total)
            lses.append(tops[h] * factors[h] + jnp.log2(total))
        o_out[dy, :, :128] = outs[0].astype(BF)
        o_out[dy, :, 128:] = jnp.where(lane < 64, outs[1], outs[2]).astype(BF)
        stats = jnp.where(lane == 0, lses[0], jnp.where(lane == 1, lses[1], lses[2]))
        st_out[dy] = jnp.transpose(stats)[:8]

    o_sends = []
    for dy in (2, 1, 3, 0):
        attend(dy)
        if dy:
            o_sends += [
                send(o_out.at[dy], o_in.at[dy], os_.at[dy], or_.at[dy], z, yp(-dy), c, x),
                send(st_out.at[dy], st_in.at[dy], ss.at[dy], sr.at[dy], z, yp(-dy), c, x),
            ]
            o_sends[-2].start()
            o_sends[-1].start()
    all_sends += o_sends

    for load in small[7:]:
        load.wait()
    eye = iota((32, 32), 0) == iota((32, 32), 1)
    before = iota((32, 32), 1) < iota((32, 32), 0)
    after = iota((32, 32), 0) < iota((32, 32), 1)
    chosen = rt[...]
    row_e = [chosen[k : k + 1].astype(F32) for k in range(2)]
    col_e = [jnp.sum(jnp.where(eye, e, 0.0), axis=1, keepdims=True) for e in row_e]
    share = wt[...]
    col_w = [
        jnp.sum(jnp.where(eye, share[k : k + 1], 0.0), axis=1, keepdims=True) for k in range(2)
    ]

    def slot(e, rank):
        e = e.astype(jnp.int32)
        dz = (e // 8 - z + NZ) % NZ
        dy = ((e // 2) % 4 - y + NY) % NY
        dc = (e % 2 - c + 2) % 2
        return dz * 16 + dy * 4 + dc * 2 + rank.astype(jnp.int32)

    row_slot, col_slot = [], []
    for k in range(2):
        rank_row = jnp.zeros((1, 32), F32)
        rank_col = jnp.zeros((32, 1), F32)
        for o in range(2):
            same = (col_e[o] == row_e[k]) & after
            rank_row = rank_row + jnp.sum(jnp.where(same, 1.0, 0.0), axis=0, keepdims=True)
            same = (row_e[o] == col_e[k]) & before
            rank_col = rank_col + jnp.sum(jnp.where(same, 1.0, 0.0), axis=1, keepdims=True)
        row_slot.append(slot(row_e[k], rank_row))
        col_slot.append(slot(col_e[k], rank_col))
    s_row = iota((128, 32), 0)
    chosen_rows = ((s_row == row_slot[0]) | (s_row == row_slot[1])).astype(BF)
    s_lane = iota((32, 128), 1)
    picks = [(s_lane == col_slot[k]).astype(BF) for k in range(2)]
    out_at, in_at = iota((128, 128), 0), iota((128, 128), 1)
    turn = (
        in_at == ((out_at // 2) % 8) * 16 + (out_at // 16) * 2 + out_at % 2
    ).astype(BF)

    for s in o_sends:
        s.wait_recv()
    lse = [jnp.transpose(st_out[0])] + [jnp.transpose(st_in[dy]) for dy in range(1, NY)]
    top = jnp.maximum(jnp.maximum(lse[0], lse[1]), jnp.maximum(lse[2], lse[3]))
    weights = [jnp.exp2(t - top) for t in lse]
    inv = 1.0 / (weights[0] + weights[1] + weights[2] + weights[3])
    sum_a = jnp.zeros((256, 128), F32)
    sum_b = jnp.zeros((256, 128), F32)
    for dy in range(NY):
        part = (o_out[0] if dy == 0 else o_in[dy]).astype(F32)
        share = weights[dy] * inv
        sum_a = sum_a + part[:, :128] * share[:, 0:1]
        sum_b = sum_b + part[:, 128:] * jnp.where(lane < 64, share[:, 1:2], share[:, 2:3])
    mg[:, :128] = sum_a.astype(BF)
    mg[:, 128:] = sum_b.astype(BF)
    swap = send(mg.at[pl.ds(high, 128)], mg_in, gs, gr, z, y, mate, x)
    swap.start()
    all_sends.append(swap)
    for load in loads[4:8]:
        load.wait()
    swap.wait_recv()
    pj[...] = (dot(mg[core_rows], wo[0]) + dot(mg_in[...], wo[1])).astype(BF)

    def rows_to(d, at, count):
        return pl.ds(pl.multiple_of(xp(d) * ROWS + at, 16), count)

    def both(a, b):
        return (a.astype(F32) + b.astype(F32)).astype(BF)

    first_up = send(pj.at[rows_to(2, 0, 16)], pj_half.at[0], ps.at[0], pr.at[0], z, y, c, up)
    first_down = send(pj.at[rows_to(2, 16, 16)], pj_half.at[1], ps.at[1], pr.at[1], z, y, c, down)
    then_up = send(pj.at[rows_to(1, 0, 32)], pj_in.at[0], ps.at[2], pr.at[2], z, y, c, up)
    then_down = send(pj.at[rows_to(-1, 0, 32)], pj_in.at[1], ps.at[3], pr.at[3], z, y, c, down)
    first_up.start()
    first_down.start()
    first_up.wait_recv()
    pj[rows_to(1, 0, 16)] = both(pj[rows_to(1, 0, 16)], pj_half[0])
    then_up.start()
    first_down.wait_recv()
    pj[rows_to(-1, 16, 16)] = both(pj[rows_to(-1, 16, 16)], pj_half[1])
    then_down.start()
    all_sends += [first_up, first_down, then_up, then_down]
    total = res[...].astype(F32) + pj[rows_to(0, 0, 32)].astype(F32)
    then_up.wait_recv()
    then_down.wait_recv()
    total = total + pj_in[0].astype(F32) + pj_in[1].astype(F32)
    hidden = total.astype(BF)
    res[...] = hidden
    v = hidden.astype(F32)
    v = v * lax.rsqrt(jnp.mean(v * v, axis=1, keepdims=True) + EPSILON)
    normed = (v * fg[...]).astype(BF)

    blocks = [(dy, dc) for dy in range(NY) for dc in range(2)]
    z_order = (4, 3, 5, 2, 6, 1, 7)
    b_order = (4, 5, 2, 3, 6, 7, 1)

    def b16(i):
        return pl.ds(i * 16, 16)

    dz = [[None] * 8 for _ in range(CHUNKS)]
    dy_ = [[None] * 8 for _ in range(CHUNKS)]
    dx = [None] * CHUNKS
    for j in range(CHUNKS):
        for d in range(1, 8):
            dz[j][d] = send(
                disp.at[j, b16(d)], z_in.at[j, b16(d)], dzs.at[j, d], dzr.at[j, d], zp(d), y, c, x
            )
            py, pc = blocks[d]
            dy_[j][d] = send(
                y_out.at[j, b16(d)], x_in.at[j, 0, b16(d)], dys.at[j, d], dyr.at[j, d],
                z, yp(py), (c + pc) % 2, x,
            )
        top_half, low_half = pl.ds(0, 64), pl.ds(64, 64)
        dx[j] = (
            send(x_in.at[j, 0], x_in.at[j, 1], dxs.at[j, 0], dxr.at[j, 0], z, y, c, up),
            send(x_in.at[j, 0], x_in.at[j, 3], dxs.at[j, 1], dxr.at[j, 1], z, y, c, down),
            send(
                x_in.at[j, 1, top_half], x_in.at[j, 2, top_half],
                dxs.at[j, 2], dxr.at[j, 2], z, y, c, up,
            ),
            send(
                x_in.at[j, 3, low_half], x_in.at[j, 2, low_half],
                dxs.at[j, 3], dxr.at[j, 3], z, y, c, down,
            ),
        )
        all_sends += dz[j][1:] + dy_[j][1:] + list(dx[j])

    for j in range(CHUNKS):
        disp[j] = dot(chosen_rows, normed[:, j * WIDE : (j + 1) * WIDE]).astype(BF)
        for d in z_order:
            dz[j][d].start()
        z_in[j, :16] = disp[j, :16]

    for t in range(CHUNKS + 2):
        if t < CHUNKS:
            for d in z_order:
                dz[t][d].wait_recv()
            y_out[t] = dot(turn, z_in[t]).astype(BF)
            for d in b_order:
                dy_[t][d].start()
            x_in[t, 0, :16] = y_out[t, :16]
        if 1 <= t <= CHUNKS:
            j = t - 1
            for d in b_order:
                dy_[j][d].wait_recv()
            dx[j][0].start()
            dx[j][1].start()
        if t == 2:
            loads[8].wait()
            loads[9].wait()
        if t >= 2:
            j = t - 2
            dx[j][0].wait_recv()
            dx[j][2].start()
            dx[j][1].wait_recv()
            dx[j][3].start()
            dx[j][2].wait_recv()
            dx[j][3].wait_recv()
            arrived = x_in[j].reshape(512, WIDE)
            g = dot(arrived, wg[j * WIDE : (j + 1) * WIDE])
            u = dot(arrived, wu[j * WIDE : (j + 1) * WIDE])
            if j == 0:
                acc_g[...] = g
                acc_u[...] = u
            elif j < CHUNKS - 1:
                acc_g[...] += g
                acc_u[...] += u
            else:
                g = acc_g[...] + g
                act[...] = (g / (1.0 + jnp.exp(-g)) * (acc_u[...] + u)).astype(BF)

    rx = [None] * CHUNKS
    ry = [[None] * 8 for _ in range(CHUNKS)]
    rz = [[None] * 8 for _ in range(CHUNKS)]
    for j in range(CHUNKS):
        rx[j] = (
            send(p_out.at[j, 2, pl.ds(0, 64)], p_half.at[j, 0], rxs.at[j, 0], rxr.at[j, 0], z, y, c, up),
            send(p_out.at[j, 2, pl.ds(64, 64)], p_half.at[j, 1], rxs.at[j, 1], rxr.at[j, 1], z, y, c, down),
            send(p_out.at[j, 3], p_in.at[j, 0], rxs.at[j, 2], rxr.at[j, 2], z, y, c, up),
            send(p_out.at[j, 1], p_in.at[j, 1], rxs.at[j, 3], rxr.at[j, 3], z, y, c, down),
        )
        for d in range(1, 8):
            py, pc = blocks[d]
            ry[j][d] = send(
                r_sum.at[j, b16(d)], ry_in.at[j, b16(d)], rys.at[j, d], ryr.at[j, d],
                z, yp(-py), (c + pc) % 2, x,
            )
            rz[j][d] = send(
                rz_out.at[j, b16(d)], rz_in.at[j, b16(d)], rzs.at[j, d], rzr.at[j, d],
                zp(-d), y, c, x,
            )
        all_sends += list(rx[j]) + ry[j][1:] + rz[j][1:]

    loads[10].wait()
    for t in range(CHUNKS + 4):
        if t < CHUNKS:
            part = dot(act[...], wd[:, t * WIDE : (t + 1) * WIDE]).astype(BF)
            p_out[t] = part.reshape(4, 128, WIDE)
            rx[t][0].start()
            rx[t][1].start()
        if 1 <= t <= CHUNKS:
            j = t - 1
            rx[j][0].wait_recv()
            p_out[j, 3, :64] = both(p_out[j, 3, :64], p_half[j, 0])
            rx[j][2].start()
            rx[j][1].wait_recv()
            p_out[j, 1, 64:] = both(p_out[j, 1, 64:], p_half[j, 1])
            rx[j][3].start()
        if 2 <= t <= CHUNKS + 1:
            j = t - 2
            rx[j][2].wait_recv()
            rx[j][3].wait_recv()
            total = p_out[j, 0].astype(F32) + p_in[j, 0].astype(F32) + p_in[j, 1].astype(F32)
            r_sum[j] = total.astype(BF)
            for d in b_order:
                ry[j][d].start()
            ry_in[j, :16] = r_sum[j, :16]
        if 3 <= t <= CHUNKS + 2:
            j = t - 3
            for d in b_order:
                ry[j][d].wait_recv()
            rz_out[j] = dot(turn, ry_in[j]).astype(BF)
            for d in z_order:
                rz[j][d].start()
            rz_in[j, :16] = rz_out[j, :16]
        if t >= 4:
            j = t - 4
            for d in z_order:
                rz[j][d].wait_recv()
            back = rz_in[j]
            mixed = col_w[0] * dot(picks[0], back) + col_w[1] * dot(picks[1], back)
            cols = slice(j * WIDE, (j + 1) * WIDE)
            out_ref[:, cols] = (res[:, cols].astype(F32) + mixed).astype(BF)

    for s in all_sends:
        s.wait_send()


def body(
    query_a, query_b, latent, rope_key, latent_gain, key_a_weight, value_a_weight, key_b_weight,
    value_b_weight, out_a_weight, out_b_weight, residual, ffn_gain, routes, route_weight,
    expert_gate, expert_up, expert_down,
):
    hbm = pl.BlockSpec(memory_space=pltpu.HBM)
    dma = pltpu.SemaphoreType.DMA
    vm = pltpu.VMEM
    ta, tb = angle_tables()
    return pl.pallas_call(
        layer_kernel,
        out_shape=jax.ShapeDtypeStruct(residual.shape, BF),
        in_specs=[hbm] * 20,
        out_specs=pl.BlockSpec(memory_space=pltpu.VMEM),
        scratch_shapes=[
            vm((128, 384), BF), vm((128, 512), BF), vm((32, 512), BF), vm((32, 64), BF),
            vm((1, 512), F32), vm((32, 2048), BF), vm((1, 2048), F32),
            vm((2, 32), jnp.int32), vm((2, 32), F32), vm((64, 256), F32), vm((128, 256), F32),
            vm((32, 640), BF), vm((2, 128, 512), BF), vm((8, 256, 640), BF), vm((4, 256, 512), BF),
            vm((512, 512), BF), vm((2, 256, 2048), BF),
            vm((8, 256, 256), BF), vm((8, 256, 128), BF), vm((8, 256, 128), BF),
            vm((8, 256, 256), BF), vm((3, 8, 256, 256), F32),
            vm((4, 256, 256), BF), vm((4, 256, 256), BF), vm((4, 8, 256), F32), vm((4, 8, 256), F32),
            vm((256, 256), BF), vm((128, 256), BF), vm((128, 2048), BF),
            vm((2, 16, 2048), BF), vm((2, 32, 2048), BF),
            vm((2048, 768), BF), vm((2048, 768), BF), vm((768, 2048), BF),
            vm((CHUNKS, 128, WIDE), BF), vm((CHUNKS, 128, WIDE), BF), vm((CHUNKS, 128, WIDE), BF),
            vm((CHUNKS, 4, 128, WIDE), BF), vm((512, 768), F32), vm((512, 768), F32),
            vm((512, 768), BF), vm((CHUNKS, 4, 128, WIDE), BF), vm((CHUNKS, 2, 64, WIDE), BF),
            vm((CHUNKS, 2, 128, WIDE), BF), vm((CHUNKS, 128, WIDE), BF),
            vm((CHUNKS, 128, WIDE), BF), vm((CHUNKS, 128, WIDE), BF), vm((CHUNKS, 128, WIDE), BF),
            dma((11,)), dma((11,)),
            dma((8,)), dma((8,)), dma((8, 4)), dma((8, 4)), dma((8,)), dma((8,)),
            dma((2, 5)), dma((2, 5)), dma((4,)), dma((4,)), dma((4,)), dma((4,)), dma, dma,
            dma((4,)), dma((4,)),
            dma((CHUNKS, 8)), dma((CHUNKS, 8)), dma((CHUNKS, 8)), dma((CHUNKS, 8)),
            dma((CHUNKS, 4)), dma((CHUNKS, 4)), dma((CHUNKS, 4)), dma((CHUNKS, 4)),
            dma((CHUNKS, 8)), dma((CHUNKS, 8)), dma((CHUNKS, 8)), dma((CHUNKS, 8)),
        ],
        compiler_params=pltpu.CompilerParams(
            collective_id=0, has_side_effects=True, vmem_limit_bytes=67043328
        ),
        cost_estimate=pl.CostEstimate(
            flops=2 * 10**10, bytes_accessed=2 * 10**7, transcendentals=10**7
        ),
    )(
        query_a, query_b, latent, rope_key, latent_gain.reshape(1, -1), key_a_weight,
        value_a_weight, key_b_weight, value_b_weight, out_a_weight, out_b_weight, residual,
        ffn_gain.reshape(1, -1), routes.T, route_weight.T, expert_gate, expert_up, expert_down,
        jnp.asarray(ta), jnp.asarray(tb),
    )


def solution(mesh):
    placed = (
        P("sp", "tp"),
        P("sp", "tp"),
        P(("sp", "tp"), None),
        P(("sp", "tp"), None),
        P(),
        P(None, "tp"),
        P(None, "tp"),
        P(None, "tp"),
        P(None, "tp"),
        P("tp", None),
        P("tp", None),
        P(("sp", "tp"), None),
        P(),
        P(("sp", "tp"), None),
        P(("sp", "tp"), None),
        P("sp", None, "tp"),
        P("sp", None, "tp"),
        P("sp", "tp", None),
    )
    return jax.shard_map(
        body, mesh=mesh, in_specs=placed, out_specs=P(("sp", "tp"), None), check_vma=False
    )
```

```python
import functools

import jax
import jax.numpy as jnp
import numpy as np
from jax import lax
from jax.experimental import pallas as pl
from jax.experimental.pallas import tpu as pltpu
from jax.sharding import PartitionSpec as P

NZ, NY, NX = 8, 4, 4
TOKENS_PER_SP = 128
ROWS = 32
OUT = ((0, 512), (512, 512), (1024, 512), (None, 128), (1536, 512))
BACK = ((0, 512), (512, 512), (1024, 512), (1536, 256), (1792, 256))
LOG2E = 1.4426950408889634
EPSILON = 1e-06
BASE_THETA = 500000.0
MASKED = -1e30
MESH_ID = pl.DeviceIdType.MESH
BF, F32 = jnp.bfloat16, jnp.float32


def angle_tables():
    inverse = BASE_THETA ** (-np.arange(0, 64, 2, dtype=np.float64) / 64)
    lanes = np.tile(inverse, 4)[None, :]

    def table(positions):
        angles = positions[:, None] * lanes
        return np.concatenate([np.cos(angles), np.sin(angles)], axis=1).astype(np.float32)

    return table(np.arange(64) * 128.0), table(np.arange(128) * 1.0)


def send(src, dst, send_sem, recv_sem, z, y, c, x):
    return pltpu.make_async_remote_copy(
        src_ref=src,
        dst_ref=dst,
        send_sem=send_sem,
        recv_sem=recv_sem,
        device_id=(z * 8 + y * 2 + c, x),
        device_id_type=MESH_ID,
    )


def dot(a, b):
    return jnp.dot(a, b, preferred_element_type=F32)


def nt_dot(a, b):
    return lax.dot_general(a, b, (((1,), (1,)), ((), ())), preferred_element_type=F32)


def iota(shape, dim):
    return lax.broadcasted_iota(jnp.int32, shape, dim)


def layer_kernel(
    qa_ref, qb_ref, lat_ref, rope_ref, gain_ref, ka_ref, va_ref, kb_ref, vb_ref, oa_ref, ob_ref,
    res_ref, fg_ref, rt_ref, wt_ref, eg_ref, eu_ref, ed_ref, ta_ref, tb_ref,
    out_ref,
    qa, qb, lat, rope, gain, res, fg, rt, wt, ta, tb,
    lat_own, q_own, latg, qg, w, wo, k_a, k_b0, k_b1, val, o_out, o_in, st_out, st_in,
    tops, sums, mixes, pj, pj_in,
    wg, wu, wd, disp, z_in, y_out, x_in, acc_g, acc_u, act, p_out, p_half, p_in, r_sum, ry_in,
    rz_out, rz_in,
    in_sem, w_sem, zs, zr, xs, xr, ms, mr, qs, qr, os_, or_, ss, sr, ps, pr,
    dzs, dzr, dys, dyr, dxs, dxr, rxs, rxr, rys, ryr, rzs, rzr,
):
    sp = lax.axis_index("sp")
    x = lax.axis_index("tp")
    z, y, c = sp // 8, (sp // 2) % 4, sp % 2
    mate = 1 - c
    low = pl.multiple_of(c * 128, 128)
    high = pl.multiple_of(mate * 128, 128)
    up = (x + 1) % NX
    down = (x + NX - 1) % NX

    def zp(d):
        return (z + d + NZ) % NZ

    def yp(d):
        return (y + d + NY) % NY

    def xp(d):
        return (x + d + NX) % NX

    small = [
        pltpu.make_async_copy(src, dst, in_sem.at[i])
        for i, (src, dst) in enumerate(
            (
                (lat_ref, lat), (rope_ref, rope), (gain_ref, gain), (ta_ref, ta), (tb_ref, tb),
                (qa_ref, qa), (qb_ref, qb), (res_ref, res), (fg_ref, fg), (rt_ref, rt), (wt_ref, wt),
            )
        )
    ]
    for load in small:
        load.start()
    loads = [
        pltpu.make_async_copy(r.at[:, pl.ds(low, 128)], w.at[:, pl.ds(i * 128, 128)], w_sem.at[i])
        for i, r in enumerate((ka_ref, kb_ref, va_ref, vb_ref))
    ]
    for i, at in enumerate((low, high)):
        for j, r in enumerate((oa_ref, ob_ref)):
            loads.append(
                pltpu.make_async_copy(
                    r.at[pl.ds(at, 128), :], wo.at[i, pl.ds(j * 128, 128)], w_sem.at[4 + 2 * i + j]
                )
            )
    for i, (src, dst) in enumerate(((eg_ref, wg), (eu_ref, wu), (ed_ref, wd))):
        loads.append(pltpu.make_async_copy(src.at[0], dst, w_sem.at[8 + i]))
    for load in loads:
        load.start()

    barrier = pltpu.get_barrier_semaphore()

    def greet(pz, py, pc, px):
        pl.semaphore_signal(
            barrier, inc=1, device_id=(pz * 8 + py * 2 + pc, px), device_id_type=MESH_ID
        )

    for d in range(1, NZ):
        greet(zp(d), y, c, x)
    for d in range(1, NX):
        greet(z, y, c, xp(d))
    for dy in range(NY):
        for dc in range(2):
            if dy or dc:
                greet(z, yp(dy), (c + dc) % 2, x)

    for load in small[:5]:
        load.wait()
    v = lat[...].astype(F32)
    v = v * lax.rsqrt(jnp.mean(v * v, axis=1, keepdims=True) + EPSILON)
    lat_own[:, :512] = (v * gain[...]).astype(BF)
    base = jnp.sum(jnp.where(iota((64, 256), 0) == sp, ta[...], 0.0), axis=0, keepdims=True)
    cos_a, sin_a = base[:, :128], base[:, 128:]

    def turning(cos_b, sin_b):
        lane = iota(cos_b.shape, 1)
        sine = sin_a * cos_b + cos_a * sin_b
        return cos_a * cos_b - sin_a * sin_b, jnp.where(lane % 64 < 32, -sine, sine)

    def rotated(tile, cosine, sine):
        lane = iota(tile.shape, 1)
        other = jnp.where(
            lane % 64 < 32, pltpu.roll(tile, 96, axis=1), pltpu.roll(tile, 32, axis=1)
        )
        return tile * cosine + other * sine

    own_32 = pl.ds(pl.multiple_of(x * ROWS, ROWS), ROWS)
    cosine, sine = turning(tb[own_32, :128], tb[own_32, 128:])
    twice = (iota((64, 128), 1) % 64 == iota((64, 128), 0)).astype(BF)
    lat_own[:, 512:] = rotated(dot(rope[...], twice), cosine, sine).astype(BF)

    pl.semaphore_wait(barrier, NZ - 1 + NX - 1 + 2 * NY - 1)

    def rows_of(px, at, count):
        return pl.ds(pl.multiple_of(c * 128 + px * ROWS + at, 16), count)

    core_rows = pl.ds(low, 128)
    all_sends = []

    z_sends = [None] + [
        send(lat_own, latg.at[d, rows_of(x, 0, 32)], zs.at[d], zr.at[d], zp(d), y, c, x)
        for d in range(1, NZ)
    ]
    all_sends += z_sends[1:]

    def ring(d):
        own = lat_own if d == 0 else latg.at[d, rows_of(x, 0, 32)]
        to = latg.at[d, rows_of(x, 0, 32)]
        one = latg.at[d, rows_of(down, 0, 16)]
        two = latg.at[d, rows_of(up, 16, 16)]
        return (
            send(own, to, xs.at[d, 0], xr.at[d, 0], z, y, c, up),
            send(own, to, xs.at[d, 1], xr.at[d, 1], z, y, c, down),
            send(one, one, xs.at[d, 2], xr.at[d, 2], z, y, c, up),
            send(two, two, xs.at[d, 3], xr.at[d, 3], z, y, c, down),
        )

    x_sends = [ring(d) for d in range(NZ)]
    for d in range(NZ):
        all_sends += x_sends[d]
    x_sends[0][0].start()
    x_sends[0][1].start()
    for d in (1, 7, 2, 6, 3, 5, 4):
        z_sends[d].start()
    latg[0, rows_of(x, 0, 32)] = lat_own[...]

    small[5].wait()
    small[6].wait()
    cosine, sine = turning(tb[:, :128], tb[:, 128:])
    lane = iota((128, 128), 1)
    t1 = qa[:, 128:256]
    t2 = qa[:, 256:384]
    r1 = rotated(t1.astype(F32), cosine, sine)
    r2 = rotated(t2.astype(F32), cosine, sine)
    mixed = jnp.where(lane < 64, t2.astype(F32), t1.astype(F32))
    q_own[0, :, :128] = qa[:, :128]
    q_own[0, :, 128:256] = jnp.where(lane < 64, r1, 0.0).astype(BF)
    q_own[1, :, :128] = pltpu.roll(mixed, 64, axis=1).astype(BF)
    q_own[1, :, 128:256] = jnp.where(lane < 64, 0.0, r2).astype(BF)
    for h in range(4):
        t = qb[:, h * 128 : h * 128 + 128].astype(F32)
        t = jnp.where(lane < 64, t, rotated(t, cosine, sine))
        if h % 2:
            t = pltpu.roll(t, 64, axis=1)
        q_own[h // 2, :, 256 + (h % 2) * 128 : 384 + (h % 2) * 128] = t.astype(BF)

    q_sends = []
    for dc in range(2):
        pc = (c + dc) % 2
        there = pl.ds(pl.multiple_of(pc * 128, 128), 128)
        one = qg.at[1, pl.ds(pl.multiple_of(pc * 128, 64), 64)]
        one_to = qg.at[2, pl.ds(pl.multiple_of(pc * 128, 64), 64)]
        two = qg.at[3, pl.ds(pl.multiple_of(pc * 128 + 64, 64), 64)]
        two_to = qg.at[2, pl.ds(pl.multiple_of(pc * 128 + 64, 64), 64)]
        q_sends.append(
            (
                send(q_own.at[pc], qg.at[1, core_rows], qs.at[dc, 0], qr.at[dc, 0], z, yp(1), pc, x),
                send(q_own.at[pc], qg.at[3, core_rows], qs.at[dc, 1], qr.at[dc, 1], z, yp(-1), pc, x),
                send(one, one_to, qs.at[dc, 2], qr.at[dc, 2], z, yp(1), c, x),
                send(two, two_to, qs.at[dc, 3], qr.at[dc, 3], z, yp(-1), c, x),
            )
        )
    q_mate = send(q_own.at[mate], qg.at[0, core_rows], qs.at[0, 4], qr.at[0, 4], z, y, mate, x)
    all_sends += q_sends[0] + q_sends[1] + (q_mate,)
    for dc in range(2):
        q_sends[dc][0].start()
        q_sends[dc][1].start()
    q_mate.start()
    qg[0, core_rows] = q_own[c]

    m_sends = [
        send(latg.at[d, core_rows], latg.at[d, core_rows], ms.at[d], mr.at[d], z, y, mate, x)
        for d in range(NZ)
    ]
    all_sends += m_sends

    def forward(d):
        x_sends[d][0].wait_recv()
        x_sends[d][2].start()
        x_sends[d][1].wait_recv()
        x_sends[d][3].start()

    def to_mate(d):
        x_sends[d][2].wait_recv()
        x_sends[d][3].wait_recv()
        m_sends[d].start()

    for load in small[7:]:
        load.wait()
    eye = iota((32, 32), 0) == iota((32, 32), 1)
    before = iota((32, 32), 1) < iota((32, 32), 0)
    after = iota((32, 32), 0) < iota((32, 32), 1)
    chosen = rt[...]
    row_e = [chosen[k : k + 1].astype(F32) for k in range(2)]
    col_e = [jnp.sum(jnp.where(eye, e, 0.0), axis=1, keepdims=True) for e in row_e]
    share = wt[...]
    col_w = [
        jnp.sum(jnp.where(eye, share[k : k + 1], 0.0), axis=1, keepdims=True) for k in range(2)
    ]

    def slot(e, rank):
        e = e.astype(jnp.int32)
        dz = (e // 8 - z + NZ) % NZ
        dy = ((e // 2) % 4 - y + NY) % NY
        dc = (e % 2 - c + 2) % 2
        return dz * 16 + dy * 4 + dc * 2 + rank.astype(jnp.int32)

    row_slot, col_slot = [], []
    for k in range(2):
        rank_row = jnp.zeros((1, 32), F32)
        rank_col = jnp.zeros((32, 1), F32)
        for o in range(2):
            same = (col_e[o] == row_e[k]) & after
            rank_row = rank_row + jnp.sum(jnp.where(same, 1.0, 0.0), axis=0, keepdims=True)
            same = (row_e[o] == col_e[k]) & before
            rank_col = rank_col + jnp.sum(jnp.where(same, 1.0, 0.0), axis=1, keepdims=True)
        row_slot.append(slot(row_e[k], rank_row))
        col_slot.append(slot(col_e[k], rank_col))
    s_row = iota((128, 32), 0)
    chosen_rows = ((s_row == row_slot[0]) | (s_row == row_slot[1])).astype(BF)
    s_lane = iota((32, 128), 1)
    picks = [(s_lane == col_slot[k]).astype(BF) for k in range(2)]
    out_at, in_at = iota((128, 128), 0), iota((128, 128), 1)
    turn = (
        in_at == ((out_at // 2) % 8) * 16 + (out_at // 16) * 2 + out_at % 2
    ).astype(BF)

    lane = iota((256, 128), 1)
    lane_512 = iota((512, 128), 1)
    row = iota((512, 128), 0)
    col = iota((512, 128), 1)
    factors = (LOG2E * 192**-0.5, LOG2E * 128**-0.5, LOG2E * 128**-0.5)

    def expand(i, d):
        at = slice(i * 256, i * 256 + 256)
        block = latg[d]
        made = dot(block[:, :512], w[...]).astype(BF)
        turned = block[:, 512:]
        b = made[:, 128:256]
        k_a[at, :128] = made[:, :128]
        k_a[at, 128:] = turned
        k_b0[at] = jnp.where(lane < 64, b, turned)
        k_b1[at] = jnp.where(lane < 64, turned, b)
        val[at] = made[:, 256:]

    def attend(i, ds):
        count = 256 * len(ds)
        q = qg[pl.ds(i * 2, 2)].reshape(512, 512)

        def raw(h):
            if h == 0:
                return nt_dot(q[:, :256], k_a[:count])
            if h == 1:
                return nt_dot(q[:, 256:384], k_b0[:count])
            return nt_dot(q[:, 384:], k_b1[:count])

        later = raw(0)
        for h in range(3):
            s = later
            if h < 2:
                later = raw(h + 1)
            tiles = [s[:, t : t + 128] for t in range(0, count, 128)]
            if ds[0] == 0:
                first, second = (yp(-2 * i) - y) * 256, (yp(-2 * i - 1) - y) * 256 - 256
                last = row + jnp.where(row < 256, first, second)
                for t in range(2):
                    tiles[t] = jnp.where(last >= col + t * 128, tiles[t], MASKED)
            if len(ds) == 2:
                for t in range(2, 4):
                    tiles[t] = jnp.where(z >= ds[1], tiles[t], MASKED)
            top = functools.reduce(jnp.maximum, tiles)
            top = jnp.broadcast_to(jnp.max(top, axis=1, keepdims=True), (512, 128))
            if ds[0]:
                old = tops[i, h]
                top = jnp.maximum(top, old)
            tops[i, h] = top
            tiles = [jnp.exp2((t - top) * factors[h]) for t in tiles]
            total = functools.reduce(jnp.add, tiles)
            weights = jnp.concatenate([t.astype(BF) for t in tiles], axis=1)
            product = dot(weights, val[:count, :128] if h == 0 else val[:count, 128:])
            if ds[0]:
                kept = jnp.exp2((old - top) * factors[h])
                sums[i, h] = sums[i, h] * kept + total
                mixes[i, h] = mixes[i, h] * kept + product
            else:
                sums[i, h] = total
                mixes[i, h] = product

    def finish(i):
        outs, lses = [], []
        for h in range(3):
            total = jnp.sum(sums[i, h], axis=1, keepdims=True)
            outs.append(mixes[i, h] / total)
            lses.append(tops[i, h] * factors[h] + jnp.log2(total))
        mixed = jnp.where(lane_512 < 64, outs[1], outs[2])
        o_out[pl.ds(2 * i, 2), :, :128] = outs[0].astype(BF).reshape(2, 256, 128)
        o_out[pl.ds(2 * i, 2), :, 128:] = mixed.astype(BF).reshape(2, 256, 128)
        stats = jnp.where(lane_512 == 0, lses[0], jnp.where(lane_512 == 1, lses[1], lses[2]))
        st_out[i] = jnp.transpose(stats)[:8]

    def arrived_z(d):
        z_sends[d].wait_recv()
        x_sends[d][0].start()
        x_sends[d][1].start()

    def forward_q(dc):
        q_sends[dc][0].wait_recv()
        q_sends[dc][2].start()
        q_sends[dc][1].wait_recv()
        q_sends[dc][3].start()

    arrived_z(1)
    arrived_z(7)
    forward(0)
    arrived_z(2)
    forward(1)
    to_mate(0)
    forward_q(0)
    arrived_z(6)
    forward(7)
    to_mate(1)
    forward_q(1)
    arrived_z(3)
    forward(2)
    to_mate(7)
    arrived_z(5)
    forward(6)
    to_mate(2)
    arrived_z(4)
    forward(3)
    to_mate(6)
    forward(5)
    forward(4)
    for load in loads[:4]:
        load.wait()
    q_mate.wait_recv()
    for dc in range(2):
        q_sends[dc][2].wait_recv()
        q_sends[dc][3].wait_recv()
    for i, d in enumerate((0, 1, 2, 7)):
        m_sends[d].wait_recv()
        if d < 2:
            expand(i, d)
        else:
            pl.when(z >= d)(functools.partial(expand, i, d))

    def near(i, carried):
        pl.when(z < 2)(functools.partial(attend, i, (0, 1)))
        pl.when((z >= 2) & (z < 7))(functools.partial(attend, i, (0, 1, 2)))
        pl.when(z == 7)(functools.partial(attend, i, (0, 1, 2, 7)))

        @pl.when(i == 0)
        def _():
            to_mate(3)
            to_mate(5)
            to_mate(4)

        return carried

    lax.fori_loop(0, 2, near, 0)

    places = [(dy, dc) for dy in range(NY) for dc in range(2)]
    o_sends = [None] * 8
    st_sends = [None] * 8
    for k in range(1, 8):
        dy, dc = places[k]
        pc = (c + dc) % 2
        at = pl.multiple_of(pc * 128, 128)
        o_sends[k] = send(
            o_out.at[dy, pl.ds(at, 128)], o_in.at[k], os_.at[k], or_.at[k], z, yp(-dy), pc, x
        )
        st_sends[k] = send(
            st_out.at[dy // 2, :, pl.ds(pl.multiple_of((dy % 2) * 256 + at, 128), 128)],
            st_in.at[k], ss.at[k], sr.at[k], z, yp(-dy), pc, x,
        )
    all_sends += o_sends[1:] + st_sends[1:]

    for i, d in enumerate((3, 4, 5, 6)):
        m_sends[d].wait_recv()
        pl.when(z >= (3 if d == 4 else d))(functools.partial(expand, i, d))

    def far(t, carried):
        i = 1 - t
        pl.when((z == 3) | (z == 4))(functools.partial(attend, i, (3, 4)))
        pl.when(z == 5)(functools.partial(attend, i, (3, 4, 5)))
        pl.when(z >= 6)(functools.partial(attend, i, (3, 4, 5, 6)))
        finish(i)

        @pl.when(t == 0)
        def _():
            for k in (4, 5, 6, 7):
                o_sends[k].start()
                st_sends[k].start()

        return carried

    lax.fori_loop(0, 2, far, 0)
    for k in (2, 3, 1):
        o_sends[k].start()
        st_sends[k].start()
    for load in loads[4:8]:
        load.wait()
    for k in range(1, 8):
        o_sends[k].wait_recv()
        st_sends[k].wait_recv()

    lane = iota((128, 128), 1)
    made = []
    for dc in range(2):
        parts, lse = [], []
        for dy in range(NY):
            k = dy * 2 + dc
            parts.append(o_out[0, core_rows] if k == 0 else o_in[k])
            lse.append(jnp.transpose(st_out[0, :, core_rows] if k == 0 else st_in[k]))
        top = jnp.maximum(jnp.maximum(lse[0], lse[1]), jnp.maximum(lse[2], lse[3]))
        weights = [jnp.exp2(t - top) for t in lse]
        inv = 1.0 / (weights[0] + weights[1] + weights[2] + weights[3])
        sum_a = jnp.zeros((128, 128), F32)
        sum_b = jnp.zeros((128, 128), F32)
        for dy in range(NY):
            part = parts[dy].astype(F32)
            share = weights[dy] * inv
            sum_a = sum_a + part[:, :128] * share[:, 0:1]
            sum_b = sum_b + part[:, 128:] * jnp.where(lane < 64, share[:, 1:2], share[:, 2:3])
        joined = jnp.concatenate([sum_a.astype(BF), sum_b.astype(BF)], axis=1)
        made.append(joined)

    def rows_to(d):
        return pl.ds(pl.multiple_of(xp(d) * ROWS, ROWS), ROWS)

    def both(a, b):
        return (a.astype(F32) + b.astype(F32)).astype(BF)

    p_sends = []
    for j in range(4):
        cols = slice(j * 512, j * 512 + 512)
        pj[j] = (dot(made[0], wo[0, :, cols]) + dot(made[1], wo[1, :, cols])).astype(BF)
        p_sends.append(
            [
                send(pj.at[j, rows_to(d)], pj_in.at[j, d], ps.at[j, d], pr.at[j, d], z, y, c, xp(d))
                for d in (2, 1, 3)
            ]
        )
        for s in p_sends[j]:
            s.start()
        all_sends += p_sends[j]

    blocks = [(dy, dc) for dy in range(NY) for dc in range(2)]
    z_order = (4, 3, 5, 2, 6, 1, 7)
    b_order = (4, 5, 2, 3, 6, 7, 1)
    count = len(OUT)

    def b16(i):
        return pl.ds(i * 16, 16)

    dz = [[None] * 8 for _ in range(count)]
    dy_ = [[None] * 8 for _ in range(count)]
    dx = [None] * count
    for j in range(count):
        for d in range(1, 8):
            dz[j][d] = send(
                disp[j].at[b16(d)], z_in[j].at[b16(d)], dzs.at[j, d], dzr.at[j, d], zp(d), y, c, x
            )
            py, pc = blocks[d]
            dy_[j][d] = send(
                y_out[j].at[b16(d)], x_in[j].at[0, b16(d)], dys.at[j, d], dyr.at[j, d],
                z, yp(py), (c + pc) % 2, x,
            )
        top_half, low_half = pl.ds(0, 64), pl.ds(64, 64)
        dx[j] = (
            send(x_in[j].at[0], x_in[j].at[1], dxs.at[j, 0], dxr.at[j, 0], z, y, c, up),
            send(x_in[j].at[0], x_in[j].at[3], dxs.at[j, 1], dxr.at[j, 1], z, y, c, down),
            send(
                x_in[j].at[1, top_half], x_in[j].at[2, top_half],
                dxs.at[j, 2], dxr.at[j, 2], z, y, c, up,
            ),
            send(
                x_in[j].at[3, low_half], x_in[j].at[2, low_half],
                dxs.at[j, 3], dxr.at[j, 3], z, y, c, down,
            ),
        )
        all_sends += dz[j][1:] + dy_[j][1:] + list(dx[j])

    def dispatch(j, rows):
        disp[j][...] = dot(chosen_rows, rows).astype(BF)
        for d in z_order:
            dz[j][d].start()
        z_in[j][:16] = disp[j][:16]

    squares = jnp.zeros((ROWS, 1), F32)
    for j in range(4):
        cols = slice(j * 512, j * 512 + 512)
        total = res[:, cols].astype(F32) + pj[j, rows_to(0)].astype(F32)
        for s in p_sends[j]:
            s.wait_recv()
        for d in range(1, NX):
            total = total + pj_in[j, d].astype(F32)
        hidden = total.astype(BF)
        res[:, cols] = hidden
        total = hidden.astype(F32)
        squares = squares + jnp.sum(total * total, axis=1, keepdims=True)
        if j < 3:
            dispatch(j, hidden)
        else:
            exact = lax.rsqrt(squares * (1.0 / 2048) + EPSILON)
            terms = []
            for _ in range(3):
                terms.append(exact.astype(BF))
                exact = exact - terms[-1].astype(F32)
            lane = iota((ROWS, 128), 1)
            scales = jnp.zeros((ROWS, 128), F32)
            for k in range(3):
                scales = jnp.where(lane == k, terms[k].astype(F32), scales)
            dispatch(3, scales.astype(BF))
            dispatch(4, hidden)

    def expert_in(j):
        at, width = OUT[j]
        floats = x_in[3][...].reshape(512, 128).astype(F32)
        scale = floats[:, 0:1] + floats[:, 1:2] + floats[:, 2:3]
        arrived = x_in[j][...].reshape(512, width).astype(F32)
        arrived = (arrived * scale * fg[:, at : at + width]).astype(BF)
        g = dot(arrived, wg[at : at + width])
        u = dot(arrived, wu[at : at + width])
        if j == 0:
            acc_g[...] = g
            acc_u[...] = u
        elif j < count - 1:
            acc_g[...] += g
            acc_u[...] += u
        else:
            g = acc_g[...] + g
            act[...] = (g / (1.0 + jnp.exp(-g)) * (acc_u[...] + u)).astype(BF)

    def plane_out(j):
        for d in z_order:
            dz[j][d].wait_recv()
        y_out[j][...] = dot(turn, z_in[j][...]).astype(BF)
        for d in b_order:
            dy_[j][d].start()
        x_in[j][0, :16] = y_out[j][:16]

    def ring_out(j):
        for d in b_order:
            dy_[j][d].wait_recv()
        dx[j][0].start()
        dx[j][1].start()

    def ring_on(j):
        dx[j][0].wait_recv()
        dx[j][2].start()
        dx[j][1].wait_recv()
        dx[j][3].start()

    def ring_end(j):
        dx[j][2].wait_recv()
        dx[j][3].wait_recv()

    plane_out(0)
    plane_out(1)
    ring_out(0)
    plane_out(2)
    ring_out(1)
    ring_on(0)
    plane_out(3)
    ring_out(2)
    plane_out(4)
    ring_on(1)
    ring_out(3)
    ring_out(4)
    ring_on(2)
    ring_on(3)
    for load in loads[8:10]:
        load.wait()
    for j in range(4):
        ring_end(j)
    expert_in(0)
    ring_on(4)
    expert_in(1)
    expert_in(2)
    ring_end(4)
    expert_in(4)

    count = len(BACK)
    rx = [None] * count
    ry = [[None] * 8 for _ in range(count)]
    rz = [[None] * 8 for _ in range(count)]
    for j in range(count):
        rx[j] = (
            send(p_out[j].at[2, pl.ds(0, 64)], p_half[j].at[0], rxs.at[j, 0], rxr.at[j, 0], z, y, c, up),
            send(p_out[j].at[2, pl.ds(64, 64)], p_half[j].at[1], rxs.at[j, 1], rxr.at[j, 1], z, y, c, down),
            send(p_out[j].at[3], p_in[j].at[0], rxs.at[j, 2], rxr.at[j, 2], z, y, c, up),
            send(p_out[j].at[1], p_in[j].at[1], rxs.at[j, 3], rxr.at[j, 3], z, y, c, down),
        )
        for d in range(1, 8):
            py, pc = blocks[d]
            ry[j][d] = send(
                r_sum[j].at[b16(d)], ry_in[j].at[b16(d)], rys.at[j, d], ryr.at[j, d],
                z, yp(-py), (c + pc) % 2, x,
            )
            rz[j][d] = send(
                rz_out[j].at[b16(d)], rz_in[j].at[b16(d)], rzs.at[j, d], rzr.at[j, d],
                zp(-d), y, c, x,
            )
        all_sends += list(rx[j]) + ry[j][1:] + rz[j][1:]

    loads[10].wait()
    for t in range(count + 6):
        if t < count:
            at, width = BACK[t]
            part = dot(act[...], wd[:, at : at + width]).astype(BF)
            p_out[t][...] = part.reshape(4, 128, width)
            rx[t][0].start()
            rx[t][1].start()
        if 3 <= t <= count + 2:
            j = t - 3
            rx[j][2].wait_recv()
            rx[j][3].wait_recv()
            total = p_out[j][0].astype(F32) + p_in[j][0].astype(F32) + p_in[j][1].astype(F32)
            r_sum[j][...] = total.astype(BF)
            for d in b_order:
                ry[j][d].start()
            ry_in[j][:16] = r_sum[j][:16]
        if 4 <= t <= count + 3:
            j = t - 4
            for d in b_order:
                ry[j][d].wait_recv()
            rz_out[j][...] = dot(turn, ry_in[j][...]).astype(BF)
            for d in z_order:
                rz[j][d].start()
            rz_in[j][:16] = rz_out[j][:16]
        if 1 <= t <= count:
            j = t - 1
            rx[j][0].wait_recv()
            p_out[j][3, :64] = both(p_out[j][3, :64], p_half[j][0])
            rx[j][2].start()
            rx[j][1].wait_recv()
            p_out[j][1, 64:] = both(p_out[j][1, 64:], p_half[j][1])
            rx[j][3].start()
        if t >= 6:
            j = t - 6
            at, width = BACK[j]
            cols = slice(at, at + width)
            for d in z_order:
                rz[j][d].wait_recv()
            back = rz_in[j][...]
            mixed = col_w[0] * dot(picks[0], back) + col_w[1] * dot(picks[1], back)
            out_ref[:, cols] = (res[:, cols].astype(F32) + mixed).astype(BF)

    for s in all_sends:
        s.wait_send()


def body(
    query_a, query_b, latent, rope_key, latent_gain, key_a_weight, value_a_weight, key_b_weight,
    value_b_weight, out_a_weight, out_b_weight, residual, ffn_gain, routes, route_weight,
    expert_gate, expert_up, expert_down,
):
    hbm = pl.BlockSpec(memory_space=pltpu.HBM)
    dma = pltpu.SemaphoreType.DMA
    vm = pltpu.VMEM
    ta, tb = angle_tables()

    def pieces(columns, *rows):
        return [vm((*rows, width), BF) for _, width in columns]

    return pl.pallas_call(
        layer_kernel,
        out_shape=jax.ShapeDtypeStruct(residual.shape, BF),
        in_specs=[hbm] * 20,
        out_specs=pl.BlockSpec(memory_space=pltpu.VMEM),
        scratch_shapes=[
            vm((128, 384), BF), vm((128, 512), BF), vm((32, 512), BF), vm((32, 64), BF),
            vm((1, 512), F32), vm((32, 2048), BF), vm((1, 2048), F32),
            vm((2, 32), jnp.int32), vm((2, 32), F32), vm((64, 256), F32), vm((128, 256), F32),
            vm((32, 640), BF), vm((2, 128, 512), BF), vm((8, 256, 640), BF), vm((4, 256, 512), BF),
            vm((512, 512), BF), vm((2, 256, 2048), BF),
            vm((1024, 256), BF), vm((1024, 128), BF), vm((1024, 128), BF), vm((1024, 256), BF),
            vm((4, 256, 256), BF), vm((8, 128, 256), BF), vm((2, 8, 512), F32), vm((8, 8, 128), F32),
            vm((2, 3, 512, 128), F32), vm((2, 3, 512, 128), F32), vm((2, 3, 512, 128), F32),
            vm((4, 128, 512), BF), vm((4, 4, 32, 512), BF),
            vm((2048, 768), BF), vm((2048, 768), BF), vm((768, 2048), BF),
            pieces(OUT, 128), pieces(OUT, 128), pieces(OUT, 128), pieces(OUT, 4, 128),
            vm((512, 768), F32), vm((512, 768), F32), vm((512, 768), BF),
            pieces(BACK, 4, 128), pieces(BACK, 2, 64), pieces(BACK, 2, 128), pieces(BACK, 128),
            pieces(BACK, 128), pieces(BACK, 128), pieces(BACK, 128),
            dma((11,)), dma((11,)),
            dma((8,)), dma((8,)), dma((8, 4)), dma((8, 4)), dma((8,)), dma((8,)),
            dma((2, 5)), dma((2, 5)), dma((8,)), dma((8,)), dma((8,)), dma((8,)),
            dma((4, 4)), dma((4, 4)),
            dma((5, 8)), dma((5, 8)), dma((5, 8)), dma((5, 8)), dma((5, 4)), dma((5, 4)),
            dma((5, 4)), dma((5, 4)), dma((5, 8)), dma((5, 8)), dma((5, 8)), dma((5, 8)),
        ],
        compiler_params=pltpu.CompilerParams(
            collective_id=0, has_side_effects=True, vmem_limit_bytes=67043328
        ),
        cost_estimate=pl.CostEstimate(
            flops=2 * 10**10, bytes_accessed=2 * 10**7, transcendentals=10**7
        ),
    )(
        query_a, query_b, latent, rope_key, latent_gain.reshape(1, -1), key_a_weight,
        value_a_weight, key_b_weight, value_b_weight, out_a_weight, out_b_weight, residual,
        ffn_gain.reshape(1, -1), routes.T, route_weight.T, expert_gate, expert_up, expert_down,
        jnp.asarray(ta), jnp.asarray(tb),
    )


def solution(mesh):
    placed = (
        P("sp", "tp"),
        P("sp", "tp"),
        P(("sp", "tp"), None),
        P(("sp", "tp"), None),
        P(),
        P(None, "tp"),
        P(None, "tp"),
        P(None, "tp"),
        P(None, "tp"),
        P("tp", None),
        P("tp", None),
        P(("sp", "tp"), None),
        P(),
        P(("sp", "tp"), None),
        P(("sp", "tp"), None),
        P("sp", None, "tp"),
        P("sp", None, "tp"),
        P("sp", "tp", None),
    )
    return jax.shard_map(
        body, mesh=mesh, in_specs=placed, out_specs=P(("sp", "tp"), None), check_vma=False
    )
```

```python
import functools

import jax
import jax.numpy as jnp
import numpy as np
from jax import lax
from jax.experimental import pallas as pl
from jax.experimental.pallas import tpu as pltpu
from jax.sharding import PartitionSpec as P

NZ, NY, NX = 8, 4, 4
TOKENS_PER_SP = 128
ROWS = 32
OUT = ((0, 256), (256, 512), (768, 512), (1280, 512), (None, 128), (1792, 256))
BACK = ((0, 256), (256, 512), (768, 512), (1280, 512), (1792, 256))
LOG2E = 1.4426950408889634
EPSILON = 1e-06
BASE_THETA = 500000.0
MASKED = -1e30
MESH_ID = pl.DeviceIdType.MESH
BF, F32 = jnp.bfloat16, jnp.float32


def angle_tables():
    inverse = BASE_THETA ** (-np.arange(0, 64, 2, dtype=np.float64) / 64)
    lanes = np.tile(inverse, 4)[None, :]

    def table(positions):
        angles = positions[:, None] * lanes
        return np.concatenate([np.cos(angles), np.sin(angles)], axis=1).astype(np.float32)

    return table(np.arange(64) * 128.0), table(np.arange(128) * 1.0)


def send(src, dst, send_sem, recv_sem, z, y, c, x):
    return pltpu.make_async_remote_copy(
        src_ref=src,
        dst_ref=dst,
        send_sem=send_sem,
        recv_sem=recv_sem,
        device_id=(z * 8 + y * 2 + c, x),
        device_id_type=MESH_ID,
    )


def dot(a, b):
    return jnp.dot(a, b, preferred_element_type=F32)


def nt_dot(a, b):
    return lax.dot_general(a, b, (((1,), (1,)), ((), ())), preferred_element_type=F32)


def iota(shape, dim):
    return lax.broadcasted_iota(jnp.int32, shape, dim)


def layer_kernel(
    qa_ref, qb_ref, lat_ref, rope_ref, gain_ref, ka_ref, va_ref, kb_ref, vb_ref, oa_ref, ob_ref,
    res_ref, fg_ref, rt_ref, wt_ref, eg_ref, eu_ref, ed_ref, ta_ref, tb_ref,
    out_ref,
    qa, qb, lat, rope, gain, res, fg, rt, wt, ta, tb,
    lat_own, q_own, latg, qg, w, wo, k_a, k_b0, k_b1, val, o_out, o_in, st_out, st_in,
    tops, sums, mixes, pj, pj_in,
    wg, wu, wd, disp, z_in, y_out, x_in, acc_g, acc_u, act, p_out, p_half, p_in, r_sum, ry_in,
    rz_out, rz_in,
    in_sem, w_sem, zs, zr, xs, xr, ms, mr, qs, qr, os_, or_, ss, sr, ps, pr,
    dzs, dzr, dys, dyr, dxs, dxr, rxs, rxr, rys, ryr, rzs, rzr,
):
    sp = lax.axis_index("sp")
    x = lax.axis_index("tp")
    z, y, c = sp // 8, (sp // 2) % 4, sp % 2
    mate = 1 - c
    low = pl.multiple_of(c * 128, 128)
    high = pl.multiple_of(mate * 128, 128)
    up = (x + 1) % NX
    down = (x + NX - 1) % NX

    def zp(d):
        return (z + d + NZ) % NZ

    def yp(d):
        return (y + d + NY) % NY

    def xp(d):
        return (x + d + NX) % NX

    small = [
        pltpu.make_async_copy(src, dst, in_sem.at[i])
        for i, (src, dst) in enumerate(
            (
                (lat_ref, lat), (rope_ref, rope), (gain_ref, gain), (ta_ref, ta), (tb_ref, tb),
                (qa_ref, qa), (qb_ref, qb), (res_ref, res), (fg_ref, fg), (rt_ref, rt), (wt_ref, wt),
            )
        )
    ]
    for load in small:
        load.start()
    loads = [
        pltpu.make_async_copy(r.at[:, pl.ds(low, 128)], w.at[:, pl.ds(i * 128, 128)], w_sem.at[i])
        for i, r in enumerate((ka_ref, kb_ref, va_ref, vb_ref))
    ]
    for i, at in enumerate((low, high)):
        for j, r in enumerate((oa_ref, ob_ref)):
            loads.append(
                pltpu.make_async_copy(
                    r.at[pl.ds(at, 128), :], wo.at[i, pl.ds(j * 128, 128)], w_sem.at[4 + 2 * i + j]
                )
            )
    for i, (src, dst) in enumerate(((eg_ref, wg), (eu_ref, wu), (ed_ref, wd))):
        loads.append(pltpu.make_async_copy(src.at[0], dst, w_sem.at[8 + i]))
    for load in loads:
        load.start()

    barrier = pltpu.get_barrier_semaphore()

    def greet(pz, py, pc, px):
        pl.semaphore_signal(
            barrier, inc=1, device_id=(pz * 8 + py * 2 + pc, px), device_id_type=MESH_ID
        )

    for d in range(1, NZ):
        greet(zp(d), y, c, x)
    for d in range(1, NX):
        greet(z, y, c, xp(d))
    for dy in range(NY):
        for dc in range(2):
            if dy or dc:
                greet(z, yp(dy), (c + dc) % 2, x)

    for load in small[:5]:
        load.wait()
    v = lat[...].astype(F32)
    v = v * lax.rsqrt(jnp.mean(v * v, axis=1, keepdims=True) + EPSILON)
    lat_own[:, :512] = (v * gain[...]).astype(BF)
    base = jnp.sum(jnp.where(iota((64, 256), 0) == sp, ta[...], 0.0), axis=0, keepdims=True)
    cos_a, sin_a = base[:, :128], base[:, 128:]

    def turning(cos_b, sin_b):
        lane = iota(cos_b.shape, 1)
        sine = sin_a * cos_b + cos_a * sin_b
        return cos_a * cos_b - sin_a * sin_b, jnp.where(lane % 64 < 32, -sine, sine)

    def rotated(tile, cosine, sine):
        lane = iota(tile.shape, 1)
        other = jnp.where(
            lane % 64 < 32, pltpu.roll(tile, 96, axis=1), pltpu.roll(tile, 32, axis=1)
        )
        return tile * cosine + other * sine

    own_32 = pl.ds(pl.multiple_of(x * ROWS, ROWS), ROWS)
    cosine, sine = turning(tb[own_32, :128], tb[own_32, 128:])
    twice = (iota((64, 128), 1) % 64 == iota((64, 128), 0)).astype(BF)
    lat_own[:, 512:] = rotated(dot(rope[...], twice), cosine, sine).astype(BF)

    pl.semaphore_wait(barrier, NZ - 1 + NX - 1 + 2 * NY - 1)

    def rows_of(px, at, count):
        return pl.ds(pl.multiple_of(c * 128 + px * ROWS + at, 16), count)

    core_rows = pl.ds(low, 128)
    all_sends = []

    z_sends = [None] + [
        send(lat_own, latg.at[d, rows_of(x, 0, 32)], zs.at[d], zr.at[d], zp(d), y, c, x)
        for d in range(1, NZ)
    ]
    all_sends += z_sends[1:]

    def ring(d):
        own = lat_own if d == 0 else latg.at[d, rows_of(x, 0, 32)]
        to = latg.at[d, rows_of(x, 0, 32)]
        one = latg.at[d, rows_of(down, 0, 16)]
        two = latg.at[d, rows_of(up, 16, 16)]
        return (
            send(own, to, xs.at[d, 0], xr.at[d, 0], z, y, c, up),
            send(own, to, xs.at[d, 1], xr.at[d, 1], z, y, c, down),
            send(one, one, xs.at[d, 2], xr.at[d, 2], z, y, c, up),
            send(two, two, xs.at[d, 3], xr.at[d, 3], z, y, c, down),
        )

    x_sends = [ring(d) for d in range(NZ)]
    for d in range(NZ):
        all_sends += x_sends[d]
    x_sends[0][0].start()
    x_sends[0][1].start()
    for d in (1, 7, 2, 6, 3, 5, 4):
        z_sends[d].start()
    latg[0, rows_of(x, 0, 32)] = lat_own[...]

    small[5].wait()
    small[6].wait()
    cosine, sine = turning(tb[:, :128], tb[:, 128:])
    lane = iota((128, 128), 1)
    t1 = qa[:, 128:256]
    t2 = qa[:, 256:384]
    r1 = rotated(t1.astype(F32), cosine, sine)
    r2 = rotated(t2.astype(F32), cosine, sine)
    mixed = jnp.where(lane < 64, t2.astype(F32), t1.astype(F32))
    q_own[0, :, :128] = qa[:, :128]
    q_own[0, :, 128:256] = jnp.where(lane < 64, r1, 0.0).astype(BF)
    q_own[1, :, :128] = pltpu.roll(mixed, 64, axis=1).astype(BF)
    q_own[1, :, 128:256] = jnp.where(lane < 64, 0.0, r2).astype(BF)
    for h in range(4):
        t = qb[:, h * 128 : h * 128 + 128].astype(F32)
        t = jnp.where(lane < 64, t, rotated(t, cosine, sine))
        if h % 2:
            t = pltpu.roll(t, 64, axis=1)
        q_own[h // 2, :, 256 + (h % 2) * 128 : 384 + (h % 2) * 128] = t.astype(BF)

    q_sends = []
    for dc in range(2):
        pc = (c + dc) % 2
        there = pl.ds(pl.multiple_of(pc * 128, 128), 128)
        one = qg.at[1, pl.ds(pl.multiple_of(pc * 128, 64), 64)]
        one_to = qg.at[2, pl.ds(pl.multiple_of(pc * 128, 64), 64)]
        two = qg.at[3, pl.ds(pl.multiple_of(pc * 128 + 64, 64), 64)]
        two_to = qg.at[2, pl.ds(pl.multiple_of(pc * 128 + 64, 64), 64)]
        q_sends.append(
            (
                send(q_own.at[pc], qg.at[1, core_rows], qs.at[dc, 0], qr.at[dc, 0], z, yp(1), pc, x),
                send(q_own.at[pc], qg.at[3, core_rows], qs.at[dc, 1], qr.at[dc, 1], z, yp(-1), pc, x),
                send(one, one_to, qs.at[dc, 2], qr.at[dc, 2], z, yp(1), c, x),
                send(two, two_to, qs.at[dc, 3], qr.at[dc, 3], z, yp(-1), c, x),
            )
        )
    q_mate = send(q_own.at[mate], qg.at[0, core_rows], qs.at[0, 4], qr.at[0, 4], z, y, mate, x)
    all_sends += q_sends[0] + q_sends[1] + (q_mate,)
    for dc in range(2):
        q_sends[dc][0].start()
        q_sends[dc][1].start()
    q_mate.start()
    qg[0, core_rows] = q_own[c]

    m_sends = [
        send(latg.at[d, core_rows], latg.at[d, core_rows], ms.at[d], mr.at[d], z, y, mate, x)
        for d in range(NZ)
    ]
    all_sends += m_sends

    def forward(d):
        x_sends[d][0].wait_recv()
        x_sends[d][2].start()
        x_sends[d][1].wait_recv()
        x_sends[d][3].start()

    def to_mate(d):
        x_sends[d][2].wait_recv()
        x_sends[d][3].wait_recv()
        m_sends[d].start()

    for load in small[7:]:
        load.wait()
    eye = iota((32, 32), 0) == iota((32, 32), 1)
    before = iota((32, 32), 1) < iota((32, 32), 0)
    after = iota((32, 32), 0) < iota((32, 32), 1)
    chosen = rt[...]
    row_e = [chosen[k : k + 1].astype(F32) for k in range(2)]
    col_e = [jnp.sum(jnp.where(eye, e, 0.0), axis=1, keepdims=True) for e in row_e]
    share = wt[...]
    col_w = [
        jnp.sum(jnp.where(eye, share[k : k + 1], 0.0), axis=1, keepdims=True) for k in range(2)
    ]

    def slot(e, rank):
        e = e.astype(jnp.int32)
        dz = (e // 8 - z + NZ) % NZ
        dy = ((e // 2) % 4 - y + NY) % NY
        dc = (e % 2 - c + 2) % 2
        return dz * 16 + dy * 4 + dc * 2 + rank.astype(jnp.int32)

    row_slot, col_slot = [], []
    for k in range(2):
        rank_row = jnp.zeros((1, 32), F32)
        rank_col = jnp.zeros((32, 1), F32)
        for o in range(2):
            same = (col_e[o] == row_e[k]) & after
            rank_row = rank_row + jnp.sum(jnp.where(same, 1.0, 0.0), axis=0, keepdims=True)
            same = (row_e[o] == col_e[k]) & before
            rank_col = rank_col + jnp.sum(jnp.where(same, 1.0, 0.0), axis=1, keepdims=True)
        row_slot.append(slot(row_e[k], rank_row))
        col_slot.append(slot(col_e[k], rank_col))
    s_row = iota((128, 32), 0)
    chosen_rows = ((s_row == row_slot[0]) | (s_row == row_slot[1])).astype(BF)
    s_lane = iota((32, 128), 1)
    picks = [(s_lane == col_slot[k]).astype(BF) for k in range(2)]
    out_at, in_at = iota((128, 128), 0), iota((128, 128), 1)
    turn = (
        in_at == ((out_at // 2) % 8) * 16 + (out_at // 16) * 2 + out_at % 2
    ).astype(BF)

    lane = iota((256, 128), 1)
    lane_512 = iota((512, 128), 1)
    row = iota((512, 128), 0)
    col = iota((512, 128), 1)
    factors = (LOG2E * 192**-0.5, LOG2E * 128**-0.5, LOG2E * 128**-0.5)

    def expand(i, d):
        at = slice(i * 256, i * 256 + 256)
        block = latg[d]
        made = dot(block[:, :512], w[...]).astype(BF)
        turned = block[:, 512:]
        b = made[:, 128:256]
        k_a[at, :128] = made[:, :128]
        k_a[at, 128:] = turned
        k_b0[at] = jnp.where(lane < 64, b, turned)
        k_b1[at] = jnp.where(lane < 64, turned, b)
        val[at] = made[:, 256:]

    def attend(i, ds):
        count = 256 * len(ds)
        q = qg[pl.ds(i * 2, 2)].reshape(512, 512)

        def raw(h):
            if h == 0:
                return nt_dot(q[:, :256], k_a[:count])
            if h == 1:
                return nt_dot(q[:, 256:384], k_b0[:count])
            return nt_dot(q[:, 384:], k_b1[:count])

        later = raw(0)
        for h in range(3):
            s = later
            if h < 2:
                later = raw(h + 1)
            tiles = [s[:, t : t + 128] for t in range(0, count, 128)]
            if ds[0] == 0:
                first, second = (yp(-2 * i) - y) * 256, (yp(-2 * i - 1) - y) * 256 - 256
                last = row + jnp.where(row < 256, first, second)
                for t in range(2):
                    tiles[t] = jnp.where(last >= col + t * 128, tiles[t], MASKED)
            if len(ds) == 2:
                for t in range(2, 4):
                    tiles[t] = jnp.where(z >= ds[1], tiles[t], MASKED)
            top = functools.reduce(jnp.maximum, tiles)
            top = jnp.broadcast_to(jnp.max(top, axis=1, keepdims=True), (512, 128))
            if ds[0]:
                old = tops[i, h]
                top = jnp.maximum(top, old)
            tops[i, h] = top
            tiles = [jnp.exp2((t - top) * factors[h]) for t in tiles]
            total = functools.reduce(jnp.add, tiles)
            weights = jnp.concatenate([t.astype(BF) for t in tiles], axis=1)
            product = dot(weights, val[:count, :128] if h == 0 else val[:count, 128:])
            if ds[0]:
                kept = jnp.exp2((old - top) * factors[h])
                sums[i, h] = sums[i, h] * kept + total
                mixes[i, h] = mixes[i, h] * kept + product
            else:
                sums[i, h] = total
                mixes[i, h] = product

    def finish(i):
        outs, lses = [], []
        for h in range(3):
            total = jnp.sum(sums[i, h], axis=1, keepdims=True)
            outs.append(mixes[i, h] / total)
            lses.append(tops[i, h] * factors[h] + jnp.log2(total))
        mixed = jnp.where(lane_512 < 64, outs[1], outs[2])
        o_out[pl.ds(2 * i, 2), :, :128] = outs[0].astype(BF).reshape(2, 256, 128)
        o_out[pl.ds(2 * i, 2), :, 128:] = mixed.astype(BF).reshape(2, 256, 128)
        stats = jnp.where(lane_512 == 0, lses[0], jnp.where(lane_512 == 1, lses[1], lses[2]))
        st_out[i] = jnp.transpose(stats)[:8]

    def arrived_z(d):
        z_sends[d].wait_recv()
        x_sends[d][0].start()
        x_sends[d][1].start()

    def forward_q(dc):
        q_sends[dc][0].wait_recv()
        q_sends[dc][2].start()
        q_sends[dc][1].wait_recv()
        q_sends[dc][3].start()

    arrived_z(1)
    arrived_z(7)
    forward(0)
    forward_q(0)
    forward_q(1)
    arrived_z(2)
    forward(1)
    arrived_z(6)
    forward(7)
    arrived_z(3)
    forward(2)
    arrived_z(5)
    forward(6)
    arrived_z(4)
    forward(3)
    to_mate(0)
    to_mate(1)
    forward(5)
    for load in loads[:4]:
        load.wait()
    q_mate.wait_recv()
    for dc in range(2):
        q_sends[dc][2].wait_recv()
        q_sends[dc][3].wait_recv()
    for i, d in enumerate((0, 1)):
        m_sends[d].wait_recv()
        expand(i, d)

    def near(i, carried):
        attend(i, (0, 1))

        @pl.when(i == 0)
        def _():
            to_mate(7)
            to_mate(2)
            forward(4)
            to_mate(6)

        return carried

    lax.fori_loop(0, 2, near, 0)
    for i, d in enumerate((2, 6, 7)):
        m_sends[d].wait_recv()
        pl.when(z >= d)(functools.partial(expand, i, d))

    def middle(i, carried):
        pl.when((z >= 2) & (z < 6))(functools.partial(attend, i, (2,)))
        pl.when(z == 6)(functools.partial(attend, i, (2, 6)))
        pl.when(z == 7)(functools.partial(attend, i, (2, 6, 7)))

        @pl.when(i == 0)
        def _():
            to_mate(5)
            to_mate(3)
            to_mate(4)

        return carried

    lax.fori_loop(0, 2, middle, 0)

    places = [(dy, dc) for dy in range(NY) for dc in range(2)]
    o_sends = [None] * 8
    st_sends = [None] * 8
    for k in range(1, 8):
        dy, dc = places[k]
        pc = (c + dc) % 2
        at = pl.multiple_of(pc * 128, 128)
        o_sends[k] = send(
            o_out.at[dy, pl.ds(at, 128)], o_in.at[k], os_.at[k], or_.at[k], z, yp(-dy), pc, x
        )
        st_sends[k] = send(
            st_out.at[dy // 2, :, pl.ds(pl.multiple_of((dy % 2) * 256 + at, 128), 128)],
            st_in.at[k], ss.at[k], sr.at[k], z, yp(-dy), pc, x,
        )
    all_sends += o_sends[1:] + st_sends[1:]

    for i, d in enumerate((3, 4, 5)):
        m_sends[d].wait_recv()
        pl.when(z >= (3 if d == 4 else d))(functools.partial(expand, i, d))

    def far(t, carried):
        i = 1 - t
        pl.when((z == 3) | (z == 4))(functools.partial(attend, i, (3, 4)))
        pl.when(z >= 5)(functools.partial(attend, i, (3, 4, 5)))
        finish(i)

        @pl.when(t == 0)
        def _():
            for k in (4, 5, 6, 7):
                o_sends[k].start()
                st_sends[k].start()

        return carried

    lax.fori_loop(0, 2, far, 0)
    for k in (2, 3, 1):
        o_sends[k].start()
        st_sends[k].start()
    for load in loads[4:8]:
        load.wait()
    for k in range(1, 8):
        o_sends[k].wait_recv()
        st_sends[k].wait_recv()

    lane = iota((128, 128), 1)
    made = []
    for dc in range(2):
        parts, lse = [], []
        for dy in range(NY):
            k = dy * 2 + dc
            parts.append(o_out[0, core_rows] if k == 0 else o_in[k])
            lse.append(jnp.transpose(st_out[0, :, core_rows] if k == 0 else st_in[k]))
        top = jnp.maximum(jnp.maximum(lse[0], lse[1]), jnp.maximum(lse[2], lse[3]))
        weights = [jnp.exp2(t - top) for t in lse]
        inv = 1.0 / (weights[0] + weights[1] + weights[2] + weights[3])
        sum_a = jnp.zeros((128, 128), F32)
        sum_b = jnp.zeros((128, 128), F32)
        for dy in range(NY):
            part = parts[dy].astype(F32)
            share = weights[dy] * inv
            sum_a = sum_a + part[:, :128] * share[:, 0:1]
            sum_b = sum_b + part[:, 128:] * jnp.where(lane < 64, share[:, 1:2], share[:, 2:3])
        joined = jnp.concatenate([sum_a.astype(BF), sum_b.astype(BF)], axis=1)
        made.append(joined)

    def rows_to(d):
        return pl.ds(pl.multiple_of(xp(d) * ROWS, ROWS), ROWS)

    def both(a, b):
        return (a.astype(F32) + b.astype(F32)).astype(BF)

    data = [j for j, (at, _) in enumerate(OUT) if at is not None]
    scaled = len(OUT) - 2
    p_sends = {}
    for j in data:
        cols = slice(OUT[j][0], sum(OUT[j]))
        pj[j][...] = (dot(made[0], wo[0, :, cols]) + dot(made[1], wo[1, :, cols])).astype(BF)
        p_sends[j] = [
            send(pj[j].at[rows_to(d)], pj_in[j].at[d], ps.at[j, d], pr.at[j, d], z, y, c, xp(d))
            for d in (2, 1, 3)
        ]
        for s in p_sends[j]:
            s.start()
        all_sends += p_sends[j]

    blocks = [(dy, dc) for dy in range(NY) for dc in range(2)]
    z_order = (4, 3, 5, 2, 6, 1, 7)
    b_order = (4, 5, 2, 3, 6, 7, 1)
    count = len(OUT)

    def b16(i):
        return pl.ds(i * 16, 16)

    dz = [[None] * 8 for _ in range(count)]
    dy_ = [[None] * 8 for _ in range(count)]
    dx = [None] * count
    for j in range(count):
        for d in range(1, 8):
            dz[j][d] = send(
                disp[j].at[b16(d)], z_in[j].at[b16(d)], dzs.at[j, d], dzr.at[j, d], zp(d), y, c, x
            )
            py, pc = blocks[d]
            dy_[j][d] = send(
                y_out[j].at[b16(d)], x_in[j].at[0, b16(d)], dys.at[j, d], dyr.at[j, d],
                z, yp(py), (c + pc) % 2, x,
            )
        top_half, low_half = pl.ds(0, 64), pl.ds(64, 64)
        dx[j] = [
            send(x_in[j].at[0], x_in[j].at[1], dxs.at[j, 0], dxr.at[j, 0], z, y, c, up),
            send(x_in[j].at[0], x_in[j].at[3], dxs.at[j, 1], dxr.at[j, 1], z, y, c, down),
        ]
        if j == scaled:
            dx[j].append(
                send(x_in[j].at[0], x_in[j].at[2], dxs.at[j, 2], dxr.at[j, 2], z, y, c, xp(2))
            )
        else:
            dx[j] += [
                send(
                    x_in[j].at[1, top_half], x_in[j].at[2, top_half],
                    dxs.at[j, 2], dxr.at[j, 2], z, y, c, up,
                ),
                send(
                    x_in[j].at[3, low_half], x_in[j].at[2, low_half],
                    dxs.at[j, 3], dxr.at[j, 3], z, y, c, down,
                ),
            ]
        all_sends += dz[j][1:] + dy_[j][1:] + list(dx[j])

    def dispatch(j, rows):
        disp[j][...] = dot(chosen_rows, rows).astype(BF)
        for d in z_order:
            dz[j][d].start()
        z_in[j][:16] = disp[j][:16]

    squares = jnp.zeros((ROWS, 1), F32)
    for j in data:
        cols = slice(OUT[j][0], sum(OUT[j]))
        total = res[:, cols].astype(F32) + pj[j][rows_to(0)].astype(F32)
        for s in p_sends[j]:
            s.wait_recv()
        for d in range(1, NX):
            total = total + pj_in[j][d].astype(F32)
        hidden = total.astype(BF)
        res[:, cols] = hidden
        total = hidden.astype(F32)
        squares = squares + jnp.sum(total * total, axis=1, keepdims=True)
        if j > scaled:
            exact = lax.rsqrt(squares * (1.0 / 2048) + EPSILON)
            terms = []
            for _ in range(3):
                terms.append(exact.astype(BF))
                exact = exact - terms[-1].astype(F32)
            lane = iota((ROWS, 128), 1)
            scales = jnp.zeros((ROWS, 128), F32)
            for k in range(3):
                scales = jnp.where(lane == k, terms[k].astype(F32), scales)
            dispatch(scaled, scales.astype(BF))
        dispatch(j, hidden)

    def expert_in(j):
        at, width = OUT[j]
        floats = x_in[scaled][...].reshape(512, 128).astype(F32)
        scale = floats[:, 0:1] + floats[:, 1:2] + floats[:, 2:3]
        arrived = x_in[j][...].reshape(512, width).astype(F32)
        arrived = (arrived * scale * fg[:, at : at + width]).astype(BF)
        g = dot(arrived, wg[at : at + width])
        u = dot(arrived, wu[at : at + width])
        if j == 0:
            acc_g[...] = g
            acc_u[...] = u
        elif j < count - 1:
            acc_g[...] += g
            acc_u[...] += u
        else:
            g = acc_g[...] + g
            act[...] = (g / (1.0 + jnp.exp(-g)) * (acc_u[...] + u)).astype(BF)

    def plane_out(j):
        for d in z_order:
            dz[j][d].wait_recv()
        y_out[j][...] = dot(turn, z_in[j][...]).astype(BF)
        for d in b_order:
            dy_[j][d].start()
        x_in[j][0, :16] = y_out[j][:16]

    def ring_out(j):
        for d in b_order:
            dy_[j][d].wait_recv()
        for s in dx[j] if j == scaled else dx[j][:2]:
            s.start()

    def ring_on(j):
        dx[j][0].wait_recv()
        dx[j][2].start()
        dx[j][1].wait_recv()
        dx[j][3].start()

    def scale_in(j):
        for s in dx[j]:
            s.wait_recv()
        for load in loads[8:10]:
            load.wait()

    def expert(j):
        dx[j][2].wait_recv()
        dx[j][3].wait_recv()
        expert_in(j)

    for step, j in (
        (plane_out, 0), (plane_out, 1), (ring_out, 0), (plane_out, 2), (ring_out, 1), (ring_on, 0),
        (plane_out, 3), (ring_out, 2), (plane_out, 4), (plane_out, 5), (ring_on, 1), (ring_out, 4),
        (ring_out, 3), (ring_out, 5), (ring_on, 2), (scale_in, 4), (expert, 0), (expert, 1),
        (ring_on, 3), (ring_on, 5), (expert, 2), (expert, 3), (expert, 5),
    ):
        step(j)

    count = len(BACK)
    rx = [None] * count
    ry = [[None] * 8 for _ in range(count)]
    rz = [[None] * 8 for _ in range(count)]
    for j in range(count):
        rx[j] = (
            send(p_out[j].at[2, pl.ds(0, 64)], p_half[j].at[0], rxs.at[j, 0], rxr.at[j, 0], z, y, c, up),
            send(p_out[j].at[2, pl.ds(64, 64)], p_half[j].at[1], rxs.at[j, 1], rxr.at[j, 1], z, y, c, down),
            send(p_out[j].at[3], p_in[j].at[0], rxs.at[j, 2], rxr.at[j, 2], z, y, c, up),
            send(p_out[j].at[1], p_in[j].at[1], rxs.at[j, 3], rxr.at[j, 3], z, y, c, down),
        )
        for d in range(1, 8):
            py, pc = blocks[d]
            ry[j][d] = send(
                r_sum[j].at[b16(d)], ry_in[j].at[b16(d)], rys.at[j, d], ryr.at[j, d],
                z, yp(-py), (c + pc) % 2, x,
            )
            rz[j][d] = send(
                rz_out[j].at[b16(d)], rz_in[j].at[b16(d)], rzs.at[j, d], rzr.at[j, d],
                zp(-d), y, c, x,
            )
        all_sends += list(rx[j]) + ry[j][1:] + rz[j][1:]

    loads[10].wait()
    for t in range(count + 6):
        if t < count:
            at, width = BACK[t]
            part = dot(act[...], wd[:, at : at + width]).astype(BF)
            p_out[t][...] = part.reshape(4, 128, width)
            rx[t][0].start()
            rx[t][1].start()
        if 3 <= t <= count + 2:
            j = t - 3
            rx[j][2].wait_recv()
            rx[j][3].wait_recv()
            total = p_out[j][0].astype(F32) + p_in[j][0].astype(F32) + p_in[j][1].astype(F32)
            r_sum[j][...] = total.astype(BF)
            for d in b_order:
                ry[j][d].start()
            ry_in[j][:16] = r_sum[j][:16]
        if 4 <= t <= count + 3:
            j = t - 4
            for d in b_order:
                ry[j][d].wait_recv()
            rz_out[j][...] = dot(turn, ry_in[j][...]).astype(BF)
            for d in z_order:
                rz[j][d].start()
            rz_in[j][:16] = rz_out[j][:16]
        if 1 <= t <= count:
            j = t - 1
            rx[j][0].wait_recv()
            p_out[j][3, :64] = both(p_out[j][3, :64], p_half[j][0])
            rx[j][2].start()
            rx[j][1].wait_recv()
            p_out[j][1, 64:] = both(p_out[j][1, 64:], p_half[j][1])
            rx[j][3].start()
        if t >= 6:
            j = t - 6
            at, width = BACK[j]
            cols = slice(at, at + width)
            for d in z_order:
                rz[j][d].wait_recv()
            back = rz_in[j][...]
            mixed = col_w[0] * dot(picks[0], back) + col_w[1] * dot(picks[1], back)
            out_ref[:, cols] = (res[:, cols].astype(F32) + mixed).astype(BF)

    for s in all_sends:
        s.wait_send()


def body(
    query_a, query_b, latent, rope_key, latent_gain, key_a_weight, value_a_weight, key_b_weight,
    value_b_weight, out_a_weight, out_b_weight, residual, ffn_gain, routes, route_weight,
    expert_gate, expert_up, expert_down,
):
    hbm = pl.BlockSpec(memory_space=pltpu.HBM)
    dma = pltpu.SemaphoreType.DMA
    vm = pltpu.VMEM
    ta, tb = angle_tables()

    def pieces(columns, *rows):
        return [vm((*rows, width), BF) for _, width in columns]

    return pl.pallas_call(
        layer_kernel,
        out_shape=jax.ShapeDtypeStruct(residual.shape, BF),
        in_specs=[hbm] * 20,
        out_specs=pl.BlockSpec(memory_space=pltpu.VMEM),
        scratch_shapes=[
            vm((128, 384), BF), vm((128, 512), BF), vm((32, 512), BF), vm((32, 64), BF),
            vm((1, 512), F32), vm((32, 2048), BF), vm((1, 2048), F32),
            vm((2, 32), jnp.int32), vm((2, 32), F32), vm((64, 256), F32), vm((128, 256), F32),
            vm((32, 640), BF), vm((2, 128, 512), BF), vm((8, 256, 640), BF), vm((4, 256, 512), BF),
            vm((512, 512), BF), vm((2, 256, 2048), BF),
            vm((768, 256), BF), vm((768, 128), BF), vm((768, 128), BF), vm((768, 256), BF),
            vm((4, 256, 256), BF), vm((8, 128, 256), BF), vm((2, 8, 512), F32), vm((8, 8, 128), F32),
            vm((2, 3, 512, 128), F32), vm((2, 3, 512, 128), F32), vm((2, 3, 512, 128), F32),
            pieces(OUT, 128), pieces(OUT, 4, 32),
            vm((2048, 768), BF), vm((2048, 768), BF), vm((768, 2048), BF),
            pieces(OUT, 128), pieces(OUT, 128), pieces(OUT, 128), pieces(OUT, 4, 128),
            vm((512, 768), F32), vm((512, 768), F32), vm((512, 768), BF),
            pieces(BACK, 4, 128), pieces(BACK, 2, 64), pieces(BACK, 2, 128), pieces(BACK, 128),
            pieces(BACK, 128), pieces(BACK, 128), pieces(BACK, 128),
            dma((11,)), dma((11,)),
            dma((8,)), dma((8,)), dma((8, 4)), dma((8, 4)), dma((8,)), dma((8,)),
            dma((2, 5)), dma((2, 5)), dma((8,)), dma((8,)), dma((8,)), dma((8,)),
            dma((6, 4)), dma((6, 4)),
            dma((6, 8)), dma((6, 8)), dma((6, 8)), dma((6, 8)), dma((6, 4)), dma((6, 4)),
            dma((6, 4)), dma((6, 4)), dma((6, 8)), dma((6, 8)), dma((6, 8)), dma((6, 8)),
        ],
        compiler_params=pltpu.CompilerParams(
            collective_id=0, has_side_effects=True, vmem_limit_bytes=67043328
        ),
        cost_estimate=pl.CostEstimate(
            flops=2 * 10**10, bytes_accessed=2 * 10**7, transcendentals=10**7
        ),
    )(
        query_a, query_b, latent, rope_key, latent_gain.reshape(1, -1), key_a_weight,
        value_a_weight, key_b_weight, value_b_weight, out_a_weight, out_b_weight, residual,
        ffn_gain.reshape(1, -1), routes.T, route_weight.T, expert_gate, expert_up, expert_down,
        jnp.asarray(ta), jnp.asarray(tb),
    )


def solution(mesh):
    placed = (
        P("sp", "tp"),
        P("sp", "tp"),
        P(("sp", "tp"), None),
        P(("sp", "tp"), None),
        P(),
        P(None, "tp"),
        P(None, "tp"),
        P(None, "tp"),
        P(None, "tp"),
        P("tp", None),
        P("tp", None),
        P(("sp", "tp"), None),
        P(),
        P(("sp", "tp"), None),
        P(("sp", "tp"), None),
        P("sp", None, "tp"),
        P("sp", None, "tp"),
        P("sp", "tp", None),
    )
    return jax.shard_map(
        body, mesh=mesh, in_specs=placed, out_specs=P(("sp", "tp"), None), check_vma=False
    )
```

```python
import functools

import jax
import jax.numpy as jnp
import numpy as np
from jax import lax
from jax.experimental import pallas as pl
from jax.experimental.pallas import tpu as pltpu
from jax.sharding import PartitionSpec as P

NZ, NY, NX = 8, 4, 4
TOKENS_PER_SP = 128
ROWS = 32
OUT = ((0, 256), (256, 512), (768, 512), (1280, 512), (None, 128), (1792, 256))
BACK = ((0, 256), (256, 512), (768, 512), (1280, 512), (1792, 256))
LOG2E = 1.4426950408889634
EPSILON = 1e-06
BASE_THETA = 500000.0
MASKED = -1e30
MESH_ID = pl.DeviceIdType.MESH
BF, F32 = jnp.bfloat16, jnp.float32


def angle_tables():
    inverse = BASE_THETA ** (-np.arange(0, 64, 2, dtype=np.float64) / 64)
    lanes = np.tile(inverse, 4)[None, :]

    def table(positions):
        angles = positions[:, None] * lanes
        return np.concatenate([np.cos(angles), np.sin(angles)], axis=1).astype(np.float32)

    return table(np.arange(64) * 128.0), table(np.arange(128) * 1.0)


def send(src, dst, send_sem, recv_sem, z, y, c, x):
    return pltpu.make_async_remote_copy(
        src_ref=src,
        dst_ref=dst,
        send_sem=send_sem,
        recv_sem=recv_sem,
        device_id=(z * 8 + y * 2 + c, x),
        device_id_type=MESH_ID,
    )


def dot(a, b):
    return jnp.dot(a, b, preferred_element_type=F32)


def nt_dot(a, b):
    return lax.dot_general(a, b, (((1,), (1,)), ((), ())), preferred_element_type=F32)


def iota(shape, dim):
    return lax.broadcasted_iota(jnp.int32, shape, dim)


def layer_kernel(
    qa_ref, qb_ref, lat_ref, rope_ref, gain_ref, ka_ref, va_ref, kb_ref, vb_ref, oa_ref, ob_ref,
    res_ref, fg_ref, rt_ref, wt_ref, eg_ref, eu_ref, ed_ref, ta_ref, tb_ref,
    out_ref,
    qa, qb, lat, rope, gain, res, fg, rt, wt, ta, tb,
    lat_own, q_own, latg, qg, w, wo, k_a, k_b0, k_b1, val, o_out, o_in, st_out, st_in,
    tops, sums, mixes, pj, pj_in,
    wg, wu, wd, disp, z_in, y_out, x_in, acc_g, acc_u, act, p_out, p_half, p_in, r_sum, ry_in,
    rz_out, rz_in,
    in_sem, w_sem, zs, zr, xs, xr, ms, mr, qs, qr, os_, or_, ss, sr, ps, pr,
    dzs, dzr, dys, dyr, dxs, dxr, rxs, rxr, rys, ryr, rzs, rzr,
):
    sp = lax.axis_index("sp")
    x = lax.axis_index("tp")
    z, y, c = sp // 8, (sp // 2) % 4, sp % 2
    mate = 1 - c
    low = pl.multiple_of(c * 128, 128)
    high = pl.multiple_of(mate * 128, 128)
    up = (x + 1) % NX
    down = (x + NX - 1) % NX

    def zp(d):
        return (z + d + NZ) % NZ

    def yp(d):
        return (y + d + NY) % NY

    def xp(d):
        return (x + d + NX) % NX

    small = [
        pltpu.make_async_copy(src, dst, in_sem.at[i])
        for i, (src, dst) in enumerate(
            (
                (lat_ref, lat), (rope_ref, rope), (gain_ref, gain), (ta_ref, ta), (tb_ref, tb),
                (qa_ref, qa), (qb_ref, qb), (res_ref, res), (fg_ref, fg), (rt_ref, rt), (wt_ref, wt),
            )
        )
    ]
    for load in small:
        load.start()
    loads = [
        pltpu.make_async_copy(r.at[:, pl.ds(low, 128)], w.at[:, pl.ds(i * 128, 128)], w_sem.at[i])
        for i, r in enumerate((ka_ref, kb_ref, va_ref, vb_ref))
    ]
    for i, at in enumerate((low, high)):
        for j, r in enumerate((oa_ref, ob_ref)):
            loads.append(
                pltpu.make_async_copy(
                    r.at[pl.ds(at, 128), :], wo.at[i, pl.ds(j * 128, 128)], w_sem.at[4 + 2 * i + j]
                )
            )
    for i, (src, dst) in enumerate(((eg_ref, wg), (eu_ref, wu), (ed_ref, wd))):
        loads.append(pltpu.make_async_copy(src.at[0], dst, w_sem.at[8 + i]))
    for load in loads[:4]:
        load.start()

    barrier = pltpu.get_barrier_semaphore()

    def greet(pz, py, pc, px):
        pl.semaphore_signal(
            barrier, inc=1, device_id=(pz * 8 + py * 2 + pc, px), device_id_type=MESH_ID
        )

    for d in range(1, NZ):
        greet(zp(d), y, c, x)
    for d in range(1, NX):
        greet(z, y, c, xp(d))
    for dy in range(NY):
        for dc in range(2):
            if dy or dc:
                greet(z, yp(dy), (c + dc) % 2, x)

    for load in small[:5]:
        load.wait()
    v = lat[...].astype(F32)
    v = v * lax.rsqrt(jnp.mean(v * v, axis=1, keepdims=True) + EPSILON)
    lat_own[:, :512] = (v * gain[...]).astype(BF)
    base = jnp.sum(jnp.where(iota((64, 256), 0) == sp, ta[...], 0.0), axis=0, keepdims=True)
    cos_a, sin_a = base[:, :128], base[:, 128:]

    def turning(cos_b, sin_b):
        lane = iota(cos_b.shape, 1)
        sine = sin_a * cos_b + cos_a * sin_b
        return cos_a * cos_b - sin_a * sin_b, jnp.where(lane % 64 < 32, -sine, sine)

    def rotated(tile, cosine, sine):
        lane = iota(tile.shape, 1)
        other = jnp.where(
            lane % 64 < 32, pltpu.roll(tile, 96, axis=1), pltpu.roll(tile, 32, axis=1)
        )
        return tile * cosine + other * sine

    own_32 = pl.ds(pl.multiple_of(x * ROWS, ROWS), ROWS)
    cosine, sine = turning(tb[own_32, :128], tb[own_32, 128:])
    twice = (iota((64, 128), 1) % 64 == iota((64, 128), 0)).astype(BF)
    lat_own[:, 512:] = rotated(dot(rope[...], twice), cosine, sine).astype(BF)

    pl.semaphore_wait(barrier, NZ - 1 + NX - 1 + 2 * NY - 1)

    def rows_of(px, at, count):
        return pl.ds(pl.multiple_of(c * 128 + px * ROWS + at, 16), count)

    core_rows = pl.ds(low, 128)
    all_sends = []

    z_sends = [None] + [
        send(lat_own, latg.at[d, rows_of(x, 0, 32)], zs.at[d], zr.at[d], zp(d), y, c, x)
        for d in range(1, NZ)
    ]
    all_sends += z_sends[1:]

    def ring(d):
        own = lat_own if d == 0 else latg.at[d, rows_of(x, 0, 32)]
        to = latg.at[d, rows_of(x, 0, 32)]
        one = latg.at[d, rows_of(down, 0, 16)]
        two = latg.at[d, rows_of(up, 16, 16)]
        return (
            send(own, to, xs.at[d, 0], xr.at[d, 0], z, y, c, up),
            send(own, to, xs.at[d, 1], xr.at[d, 1], z, y, c, down),
            send(one, one, xs.at[d, 2], xr.at[d, 2], z, y, c, up),
            send(two, two, xs.at[d, 3], xr.at[d, 3], z, y, c, down),
        )

    x_sends = [ring(d) for d in range(NZ)]
    for d in range(NZ):
        all_sends += x_sends[d]
    x_sends[0][0].start()
    x_sends[0][1].start()
    for d in (1, 7, 2, 6, 3, 5, 4):
        z_sends[d].start()
    latg[0, rows_of(x, 0, 32)] = lat_own[...]

    small[5].wait()
    small[6].wait()
    cosine, sine = turning(tb[:, :128], tb[:, 128:])
    lane = iota((128, 128), 1)
    t1 = qa[:, 128:256]
    t2 = qa[:, 256:384]
    r1 = rotated(t1.astype(F32), cosine, sine)
    r2 = rotated(t2.astype(F32), cosine, sine)
    mixed = jnp.where(lane < 64, t2.astype(F32), t1.astype(F32))
    q_own[0, :, :128] = qa[:, :128]
    q_own[0, :, 128:256] = jnp.where(lane < 64, r1, 0.0).astype(BF)
    q_own[1, :, :128] = pltpu.roll(mixed, 64, axis=1).astype(BF)
    q_own[1, :, 128:256] = jnp.where(lane < 64, 0.0, r2).astype(BF)
    for h in range(4):
        t = qb[:, h * 128 : h * 128 + 128].astype(F32)
        t = jnp.where(lane < 64, t, rotated(t, cosine, sine))
        if h % 2:
            t = pltpu.roll(t, 64, axis=1)
        q_own[h // 2, :, 256 + (h % 2) * 128 : 384 + (h % 2) * 128] = t.astype(BF)

    q_sends = []
    for dc in range(2):
        pc = (c + dc) % 2
        there = pl.ds(pl.multiple_of(pc * 128, 128), 128)
        one = qg.at[1, pl.ds(pl.multiple_of(pc * 128, 64), 64)]
        one_to = qg.at[2, pl.ds(pl.multiple_of(pc * 128, 64), 64)]
        two = qg.at[3, pl.ds(pl.multiple_of(pc * 128 + 64, 64), 64)]
        two_to = qg.at[2, pl.ds(pl.multiple_of(pc * 128 + 64, 64), 64)]
        q_sends.append(
            (
                send(q_own.at[pc], qg.at[1, core_rows], qs.at[dc, 0], qr.at[dc, 0], z, yp(1), pc, x),
                send(q_own.at[pc], qg.at[3, core_rows], qs.at[dc, 1], qr.at[dc, 1], z, yp(-1), pc, x),
                send(one, one_to, qs.at[dc, 2], qr.at[dc, 2], z, yp(1), c, x),
                send(two, two_to, qs.at[dc, 3], qr.at[dc, 3], z, yp(-1), c, x),
            )
        )
    q_mate = send(q_own.at[mate], qg.at[0, core_rows], qs.at[0, 4], qr.at[0, 4], z, y, mate, x)
    all_sends += q_sends[0] + q_sends[1] + (q_mate,)
    for dc in range(2):
        q_sends[dc][0].start()
        q_sends[dc][1].start()
    q_mate.start()
    for load in loads[4:]:
        load.start()
    qg[0, core_rows] = q_own[c]

    m_sends = [
        send(latg.at[d, core_rows], latg.at[d, core_rows], ms.at[d], mr.at[d], z, y, mate, x)
        for d in range(NZ)
    ]
    all_sends += m_sends

    def forward(d):
        x_sends[d][0].wait_recv()
        x_sends[d][2].start()
        x_sends[d][1].wait_recv()
        x_sends[d][3].start()

    def to_mate(d):
        x_sends[d][2].wait_recv()
        x_sends[d][3].wait_recv()
        m_sends[d].start()

    lane = iota((256, 128), 1)
    lane_512 = iota((512, 128), 1)
    row = iota((512, 128), 0)
    col = iota((512, 128), 1)
    factors = (LOG2E * 192**-0.5, LOG2E * 128**-0.5, LOG2E * 128**-0.5)

    def expand(i, d):
        at = slice(i * 256, i * 256 + 256)
        block = latg[d]
        made = dot(block[:, :512], w[...]).astype(BF)
        turned = block[:, 512:]
        b = made[:, 128:256]
        k_a[at, :128] = made[:, :128]
        k_a[at, 128:] = turned
        k_b0[at] = jnp.where(lane < 64, b, turned)
        k_b1[at] = jnp.where(lane < 64, turned, b)
        val[at] = made[:, 256:]

    def attend(i, ds):
        count = 256 * len(ds)
        q = qg[pl.ds(i * 2, 2)].reshape(512, 512)

        def raw(h):
            if h == 0:
                return nt_dot(q[:, :256], k_a[:count])
            if h == 1:
                return nt_dot(q[:, 256:384], k_b0[:count])
            return nt_dot(q[:, 384:], k_b1[:count])

        later = raw(0)
        for h in range(3):
            s = later
            if h < 2:
                later = raw(h + 1)
            tiles = [s[:, t : t + 128] for t in range(0, count, 128)]
            if ds[0] == 0:
                first, second = (yp(-2 * i) - y) * 256, (yp(-2 * i - 1) - y) * 256 - 256
                last = row + jnp.where(row < 256, first, second)
                for t in range(2):
                    tiles[t] = jnp.where(last >= col + t * 128, tiles[t], MASKED)
            if len(ds) == 2:
                for t in range(2, 4):
                    tiles[t] = jnp.where(z >= ds[1], tiles[t], MASKED)
            top = functools.reduce(jnp.maximum, tiles)
            top = jnp.broadcast_to(jnp.max(top, axis=1, keepdims=True), (512, 128))
            if ds[0]:
                old = tops[i, h]
                top = jnp.maximum(top, old)
            tops[i, h] = top
            tiles = [jnp.exp2((t - top) * factors[h]) for t in tiles]
            total = functools.reduce(jnp.add, tiles)
            weights = jnp.concatenate([t.astype(BF) for t in tiles], axis=1)
            product = dot(weights, val[:count, :128] if h == 0 else val[:count, 128:])
            if ds[0]:
                kept = jnp.exp2((old - top) * factors[h])
                sums[i, h] = sums[i, h] * kept + total
                mixes[i, h] = mixes[i, h] * kept + product
            else:
                sums[i, h] = total
                mixes[i, h] = product

    def finish(i):
        outs, lses = [], []
        for h in range(3):
            total = jnp.sum(sums[i, h], axis=1, keepdims=True)
            outs.append(mixes[i, h] / total)
            lses.append(tops[i, h] * factors[h] + jnp.log2(total))
        mixed = jnp.where(lane_512 < 64, outs[1], outs[2])
        o_out[pl.ds(2 * i, 2), :, :128] = outs[0].astype(BF).reshape(2, 256, 128)
        o_out[pl.ds(2 * i, 2), :, 128:] = mixed.astype(BF).reshape(2, 256, 128)
        stats = jnp.where(lane_512 == 0, lses[0], jnp.where(lane_512 == 1, lses[1], lses[2]))
        st_out[i] = jnp.transpose(stats)[:8]

    def arrived_z(d):
        z_sends[d].wait_recv()
        x_sends[d][0].start()
        x_sends[d][1].start()

    def forward_q(dc):
        q_sends[dc][0].wait_recv()
        q_sends[dc][2].start()
        q_sends[dc][1].wait_recv()
        q_sends[dc][3].start()

    arrived_z(1)
    arrived_z(7)
    forward(0)
    forward_q(0)
    forward_q(1)
    arrived_z(2)
    forward(1)
    arrived_z(6)
    forward(7)
    arrived_z(3)
    forward(2)
    arrived_z(5)
    forward(6)
    arrived_z(4)
    forward(3)
    to_mate(0)
    to_mate(1)
    forward(5)
    for load in loads[:4]:
        load.wait()
    q_mate.wait_recv()
    for dc in range(2):
        q_sends[dc][2].wait_recv()
        q_sends[dc][3].wait_recv()
    for i, d in enumerate((0, 1)):
        m_sends[d].wait_recv()
        expand(i, d)

    def near(i, carried):
        attend(i, (0, 1))

        @pl.when(i == 0)
        def _():
            to_mate(7)
            to_mate(2)
            forward(4)
            to_mate(6)

        return carried

    lax.fori_loop(0, 2, near, 0)
    for i, d in enumerate((2, 6, 7)):
        m_sends[d].wait_recv()
        pl.when(z >= d)(functools.partial(expand, i, d))

    def middle(i, carried):
        pl.when((z >= 2) & (z < 6))(functools.partial(attend, i, (2,)))
        pl.when(z == 6)(functools.partial(attend, i, (2, 6)))
        pl.when(z == 7)(functools.partial(attend, i, (2, 6, 7)))

        @pl.when(i == 0)
        def _():
            to_mate(5)
            to_mate(3)
            to_mate(4)

        return carried

    lax.fori_loop(0, 2, middle, 0)

    places = [(dy, dc) for dy in range(NY) for dc in range(2)]
    o_sends = [None] * 8
    st_sends = [None] * 8
    for k in range(1, 8):
        dy, dc = places[k]
        pc = (c + dc) % 2
        at = pl.multiple_of(pc * 128, 128)
        o_sends[k] = send(
            o_out.at[dy, pl.ds(at, 128)], o_in.at[k], os_.at[k], or_.at[k], z, yp(-dy), pc, x
        )
        st_sends[k] = send(
            st_out.at[dy // 2, :, pl.ds(pl.multiple_of((dy % 2) * 256 + at, 128), 128)],
            st_in.at[k], ss.at[k], sr.at[k], z, yp(-dy), pc, x,
        )
    all_sends += o_sends[1:] + st_sends[1:]

    for i, d in enumerate((3, 4, 5)):
        m_sends[d].wait_recv()
        pl.when(z >= (3 if d == 4 else d))(functools.partial(expand, i, d))

    def far(t, carried):
        i = 1 - t
        pl.when((z == 3) | (z == 4))(functools.partial(attend, i, (3, 4)))
        pl.when(z >= 5)(functools.partial(attend, i, (3, 4, 5)))
        finish(i)

        @pl.when(t == 0)
        def _():
            for k in (4, 5, 6, 7):
                o_sends[k].start()
                st_sends[k].start()

        return carried

    lax.fori_loop(0, 2, far, 0)
    for k in (2, 3, 1):
        o_sends[k].start()
        st_sends[k].start()
    for load in small[7:]:
        load.wait()
    eye = iota((32, 32), 0) == iota((32, 32), 1)
    before = iota((32, 32), 1) < iota((32, 32), 0)
    after = iota((32, 32), 0) < iota((32, 32), 1)
    chosen = rt[...]
    row_e = [chosen[k : k + 1].astype(F32) for k in range(2)]
    col_e = [jnp.sum(jnp.where(eye, e, 0.0), axis=1, keepdims=True) for e in row_e]
    share = wt[...]
    col_w = [
        jnp.sum(jnp.where(eye, share[k : k + 1], 0.0), axis=1, keepdims=True) for k in range(2)
    ]

    def slot(e, rank):
        e = e.astype(jnp.int32)
        dz = (e // 8 - z + NZ) % NZ
        dy = ((e // 2) % 4 - y + NY) % NY
        dc = (e % 2 - c + 2) % 2
        return dz * 16 + dy * 4 + dc * 2 + rank.astype(jnp.int32)

    row_slot, col_slot = [], []
    for k in range(2):
        rank_row = jnp.zeros((1, 32), F32)
        rank_col = jnp.zeros((32, 1), F32)
        for o in range(2):
            same = (col_e[o] == row_e[k]) & after
            rank_row = rank_row + jnp.sum(jnp.where(same, 1.0, 0.0), axis=0, keepdims=True)
            same = (row_e[o] == col_e[k]) & before
            rank_col = rank_col + jnp.sum(jnp.where(same, 1.0, 0.0), axis=1, keepdims=True)
        row_slot.append(slot(row_e[k], rank_row))
        col_slot.append(slot(col_e[k], rank_col))
    s_row = iota((128, 32), 0)
    chosen_rows = ((s_row == row_slot[0]) | (s_row == row_slot[1])).astype(BF)
    s_lane = iota((32, 128), 1)
    picks = [(s_lane == col_slot[k]).astype(BF) for k in range(2)]
    out_at, in_at = iota((128, 128), 0), iota((128, 128), 1)
    turn = (
        in_at == ((out_at // 2) % 8) * 16 + (out_at // 16) * 2 + out_at % 2
    ).astype(BF)

    for load in loads[4:8]:
        load.wait()
    for k in range(1, 8):
        o_sends[k].wait_recv()
        st_sends[k].wait_recv()

    lane = iota((128, 128), 1)
    made = []
    for dc in range(2):
        parts, lse = [], []
        for dy in range(NY):
            k = dy * 2 + dc
            parts.append(o_out[0, core_rows] if k == 0 else o_in[k])
            lse.append(jnp.transpose(st_out[0, :, core_rows] if k == 0 else st_in[k]))
        top = jnp.maximum(jnp.maximum(lse[0], lse[1]), jnp.maximum(lse[2], lse[3]))
        weights = [jnp.exp2(t - top) for t in lse]
        inv = 1.0 / (weights[0] + weights[1] + weights[2] + weights[3])
        sum_a = jnp.zeros((128, 128), F32)
        sum_b = jnp.zeros((128, 128), F32)
        for dy in range(NY):
            part = parts[dy].astype(F32)
            share = weights[dy] * inv
            sum_a = sum_a + part[:, :128] * share[:, 0:1]
            sum_b = sum_b + part[:, 128:] * jnp.where(lane < 64, share[:, 1:2], share[:, 2:3])
        joined = jnp.concatenate([sum_a.astype(BF), sum_b.astype(BF)], axis=1)
        made.append(joined)

    def rows_to(d):
        return pl.ds(pl.multiple_of(xp(d) * ROWS, ROWS), ROWS)

    def both(a, b):
        return (a.astype(F32) + b.astype(F32)).astype(BF)

    data = [j for j, (at, _) in enumerate(OUT) if at is not None]
    scaled = len(OUT) - 2
    p_sends = {}
    for j in data:
        cols = slice(OUT[j][0], sum(OUT[j]))
        pj[j][...] = (dot(made[0], wo[0, :, cols]) + dot(made[1], wo[1, :, cols])).astype(BF)
        p_sends[j] = [
            send(pj[j].at[rows_to(d)], pj_in[j].at[d], ps.at[j, d], pr.at[j, d], z, y, c, xp(d))
            for d in (2, 1, 3)
        ]
        for s in p_sends[j]:
            s.start()
        all_sends += p_sends[j]

    blocks = [(dy, dc) for dy in range(NY) for dc in range(2)]
    z_order = (4, 3, 5, 2, 6, 1, 7)
    b_order = (4, 5, 2, 3, 6, 7, 1)
    count = len(OUT)

    def b16(i):
        return pl.ds(i * 16, 16)

    dz = [[None] * 8 for _ in range(count)]
    dy_ = [[None] * 8 for _ in range(count)]
    dx = [None] * count
    for j in range(count):
        for d in range(1, 8):
            dz[j][d] = send(
                disp[j].at[b16(d)], z_in[j].at[b16(d)], dzs.at[j, d], dzr.at[j, d], zp(d), y, c, x
            )
            py, pc = blocks[d]
            dy_[j][d] = send(
                y_out[j].at[b16(d)], x_in[j].at[0, b16(d)], dys.at[j, d], dyr.at[j, d],
                z, yp(py), (c + pc) % 2, x,
            )
        top_half, low_half = pl.ds(0, 64), pl.ds(64, 64)
        dx[j] = [
            send(x_in[j].at[0], x_in[j].at[1], dxs.at[j, 0], dxr.at[j, 0], z, y, c, up),
            send(x_in[j].at[0], x_in[j].at[3], dxs.at[j, 1], dxr.at[j, 1], z, y, c, down),
        ]
        if j == scaled:
            dx[j].append(
                send(x_in[j].at[0], x_in[j].at[2], dxs.at[j, 2], dxr.at[j, 2], z, y, c, xp(2))
            )
        else:
            dx[j] += [
                send(
                    x_in[j].at[1, top_half], x_in[j].at[2, top_half],
                    dxs.at[j, 2], dxr.at[j, 2], z, y, c, up,
                ),
                send(
                    x_in[j].at[3, low_half], x_in[j].at[2, low_half],
                    dxs.at[j, 3], dxr.at[j, 3], z, y, c, down,
                ),
            ]
        all_sends += dz[j][1:] + dy_[j][1:] + list(dx[j])

    def dispatch(j, rows):
        disp[j][...] = dot(chosen_rows, rows).astype(BF)
        for d in z_order:
            dz[j][d].start()
        z_in[j][:16] = disp[j][:16]

    squares = jnp.zeros((ROWS, 1), F32)
    for j in data:
        cols = slice(OUT[j][0], sum(OUT[j]))
        total = res[:, cols].astype(F32) + pj[j][rows_to(0)].astype(F32)
        for s in p_sends[j]:
            s.wait_recv()
        for d in range(1, NX):
            total = total + pj_in[j][d].astype(F32)
        hidden = total.astype(BF)
        res[:, cols] = hidden
        total = hidden.astype(F32)
        squares = squares + jnp.sum(total * total, axis=1, keepdims=True)
        if j > scaled:
            exact = lax.rsqrt(squares * (1.0 / 2048) + EPSILON)
            terms = []
            for _ in range(3):
                terms.append(exact.astype(BF))
                exact = exact - terms[-1].astype(F32)
            lane = iota((ROWS, 128), 1)
            scales = jnp.zeros((ROWS, 128), F32)
            for k in range(3):
                scales = jnp.where(lane == k, terms[k].astype(F32), scales)
            dispatch(scaled, scales.astype(BF))
        dispatch(j, hidden)

    def expert_in(j):
        at, width = OUT[j]
        floats = x_in[scaled][...].reshape(512, 128).astype(F32)
        scale = floats[:, 0:1] + floats[:, 1:2] + floats[:, 2:3]
        arrived = x_in[j][...].reshape(512, width).astype(F32)
        arrived = (arrived * scale * fg[:, at : at + width]).astype(BF)
        g = dot(arrived, wg[at : at + width])
        u = dot(arrived, wu[at : at + width])
        if j == 0:
            acc_g[...] = g
            acc_u[...] = u
        elif j < count - 1:
            acc_g[...] += g
            acc_u[...] += u
        else:
            g = acc_g[...] + g
            act[...] = (g / (1.0 + jnp.exp(-g)) * (acc_u[...] + u)).astype(BF)

    def plane_out(j):
        for d in z_order:
            dz[j][d].wait_recv()
        y_out[j][...] = dot(turn, z_in[j][...]).astype(BF)
        for d in b_order:
            dy_[j][d].start()
        x_in[j][0, :16] = y_out[j][:16]

    def ring_out(j):
        for d in b_order:
            dy_[j][d].wait_recv()
        for s in dx[j] if j == scaled else dx[j][:2]:
            s.start()

    def ring_on(j):
        dx[j][0].wait_recv()
        dx[j][2].start()
        dx[j][1].wait_recv()
        dx[j][3].start()

    def scale_in(j):
        for s in dx[j]:
            s.wait_recv()
        for load in loads[8:10]:
            load.wait()

    def expert(j):
        dx[j][2].wait_recv()
        dx[j][3].wait_recv()
        expert_in(j)

    for step, j in (
        (plane_out, 0), (plane_out, 1), (ring_out, 0), (plane_out, 2), (ring_out, 1), (ring_on, 0),
        (plane_out, 3), (ring_out, 2), (plane_out, 4), (plane_out, 5), (ring_on, 1), (ring_out, 4),
        (ring_out, 3), (ring_out, 5), (ring_on, 2), (scale_in, 4), (expert, 0), (expert, 1),
        (ring_on, 3), (ring_on, 5), (expert, 2), (expert, 3), (expert, 5),
    ):
        step(j)

    count = len(BACK)
    rx = [None] * count
    ry = [[None] * 8 for _ in range(count)]
    rz = [[None] * 8 for _ in range(count)]
    for j in range(count):
        rx[j] = (
            send(p_out[j].at[2, pl.ds(0, 64)], p_half[j].at[0], rxs.at[j, 0], rxr.at[j, 0], z, y, c, up),
            send(p_out[j].at[2, pl.ds(64, 64)], p_half[j].at[1], rxs.at[j, 1], rxr.at[j, 1], z, y, c, down),
            send(p_out[j].at[3], p_in[j].at[0], rxs.at[j, 2], rxr.at[j, 2], z, y, c, up),
            send(p_out[j].at[1], p_in[j].at[1], rxs.at[j, 3], rxr.at[j, 3], z, y, c, down),
        )
        for d in range(1, 8):
            py, pc = blocks[d]
            ry[j][d] = send(
                r_sum[j].at[b16(d)], ry_in[j].at[b16(d)], rys.at[j, d], ryr.at[j, d],
                z, yp(-py), (c + pc) % 2, x,
            )
            rz[j][d] = send(
                rz_out[j].at[b16(d)], rz_in[j].at[b16(d)], rzs.at[j, d], rzr.at[j, d],
                zp(-d), y, c, x,
            )
        all_sends += list(rx[j]) + ry[j][1:] + rz[j][1:]

    loads[10].wait()
    for t in range(count + 6):
        if t < count:
            at, width = BACK[t]
            part = dot(act[...], wd[:, at : at + width]).astype(BF)
            p_out[t][...] = part.reshape(4, 128, width)
            rx[t][0].start()
            rx[t][1].start()
        if 3 <= t <= count + 2:
            j = t - 3
            rx[j][2].wait_recv()
            rx[j][3].wait_recv()
            total = p_out[j][0].astype(F32) + p_in[j][0].astype(F32) + p_in[j][1].astype(F32)
            r_sum[j][...] = total.astype(BF)
            for d in b_order:
                ry[j][d].start()
            ry_in[j][:16] = r_sum[j][:16]
        if 4 <= t <= count + 3:
            j = t - 4
            for d in b_order:
                ry[j][d].wait_recv()
            rz_out[j][...] = dot(turn, ry_in[j][...]).astype(BF)
            for d in z_order:
                rz[j][d].start()
            rz_in[j][:16] = rz_out[j][:16]
        if 1 <= t <= count:
            j = t - 1
            rx[j][0].wait_recv()
            p_out[j][3, :64] = both(p_out[j][3, :64], p_half[j][0])
            rx[j][2].start()
            rx[j][1].wait_recv()
            p_out[j][1, 64:] = both(p_out[j][1, 64:], p_half[j][1])
            rx[j][3].start()
        if t >= 6:
            j = t - 6
            at, width = BACK[j]
            cols = slice(at, at + width)
            for d in z_order:
                rz[j][d].wait_recv()
            back = rz_in[j][...]
            mixed = col_w[0] * dot(picks[0], back) + col_w[1] * dot(picks[1], back)
            out_ref[:, cols] = (res[:, cols].astype(F32) + mixed).astype(BF)

    for s in all_sends:
        s.wait_send()


def body(
    query_a, query_b, latent, rope_key, latent_gain, key_a_weight, value_a_weight, key_b_weight,
    value_b_weight, out_a_weight, out_b_weight, residual, ffn_gain, routes, route_weight,
    expert_gate, expert_up, expert_down,
):
    hbm = pl.BlockSpec(memory_space=pltpu.HBM)
    dma = pltpu.SemaphoreType.DMA
    vm = pltpu.VMEM
    ta, tb = angle_tables()

    def pieces(columns, *rows):
        return [vm((*rows, width), BF) for _, width in columns]

    return pl.pallas_call(
        layer_kernel,
        out_shape=jax.ShapeDtypeStruct(residual.shape, BF),
        in_specs=[hbm] * 20,
        out_specs=pl.BlockSpec(memory_space=pltpu.VMEM),
        scratch_shapes=[
            vm((128, 384), BF), vm((128, 512), BF), vm((32, 512), BF), vm((32, 64), BF),
            vm((1, 512), F32), vm((32, 2048), BF), vm((1, 2048), F32),
            vm((2, 32), jnp.int32), vm((2, 32), F32), vm((64, 256), F32), vm((128, 256), F32),
            vm((32, 640), BF), vm((2, 128, 512), BF), vm((8, 256, 640), BF), vm((4, 256, 512), BF),
            vm((512, 512), BF), vm((2, 256, 2048), BF),
            vm((768, 256), BF), vm((768, 128), BF), vm((768, 128), BF), vm((768, 256), BF),
            vm((4, 256, 256), BF), vm((8, 128, 256), BF), vm((2, 8, 512), F32), vm((8, 8, 128), F32),
            vm((2, 3, 512, 128), F32), vm((2, 3, 512, 128), F32), vm((2, 3, 512, 128), F32),
            pieces(OUT, 128), pieces(OUT, 4, 32),
            vm((2048, 768), BF), vm((2048, 768), BF), vm((768, 2048), BF),
            pieces(OUT, 128), pieces(OUT, 128), pieces(OUT, 128), pieces(OUT, 4, 128),
            vm((512, 768), F32), vm((512, 768), F32), vm((512, 768), BF),
            pieces(BACK, 4, 128), pieces(BACK, 2, 64), pieces(BACK, 2, 128), pieces(BACK, 128),
            pieces(BACK, 128), pieces(BACK, 128), pieces(BACK, 128),
            dma((11,)), dma((11,)),
            dma((8,)), dma((8,)), dma((8, 4)), dma((8, 4)), dma((8,)), dma((8,)),
            dma((2, 5)), dma((2, 5)), dma((8,)), dma((8,)), dma((8,)), dma((8,)),
            dma((6, 4)), dma((6, 4)),
            dma((6, 8)), dma((6, 8)), dma((6, 8)), dma((6, 8)), dma((6, 4)), dma((6, 4)),
            dma((6, 4)), dma((6, 4)), dma((6, 8)), dma((6, 8)), dma((6, 8)), dma((6, 8)),
        ],
        compiler_params=pltpu.CompilerParams(
            collective_id=0, has_side_effects=True, vmem_limit_bytes=67043328
        ),
        cost_estimate=pl.CostEstimate(
            flops=2 * 10**10, bytes_accessed=2 * 10**7, transcendentals=10**7
        ),
    )(
        query_a, query_b, latent, rope_key, latent_gain.reshape(1, -1), key_a_weight,
        value_a_weight, key_b_weight, value_b_weight, out_a_weight, out_b_weight, residual,
        ffn_gain.reshape(1, -1), routes.T, route_weight.T, expert_gate, expert_up, expert_down,
        jnp.asarray(ta), jnp.asarray(tb),
    )


def solution(mesh):
    placed = (
        P("sp", "tp"),
        P("sp", "tp"),
        P(("sp", "tp"), None),
        P(("sp", "tp"), None),
        P(),
        P(None, "tp"),
        P(None, "tp"),
        P(None, "tp"),
        P(None, "tp"),
        P("tp", None),
        P("tp", None),
        P(("sp", "tp"), None),
        P(),
        P(("sp", "tp"), None),
        P(("sp", "tp"), None),
        P("sp", None, "tp"),
        P("sp", None, "tp"),
        P("sp", "tp", None),
    )
    return jax.shard_map(
        body, mesh=mesh, in_specs=placed, out_specs=P(("sp", "tp"), None), check_vma=False
    )
```
